32 devices in a mesh: grp: 2 (over y), fs: 4 (over z), tp: 4 (over x, core).
Axes of the slice: x: 2, y: 2, z: 4, core: 2. Of those that a mesh axis runs over, the one named last changes fastest.
Arguments:
- tokens: bfloat16 [2048, 3072], P(('grp', 'tp')), parts along dimension 0, may hold values from -6 to 6
- up_master: float32 [3072, 12288], P('fs', 'tp'), may hold values from -0.109375 to 0.109375
- down_master: float32 [12288, 3072], P('fs', 'tp'), may hold values from -0.0546875 to 0.0546875
- norm_gain: float32 [3072], P('fs'), may hold values from 0.1 to 1.9
Outputs:
- prompt_out: bfloat16 [2048, 3072], P(('grp', 'tp'), 'fs'), parts along dimension 0
- sampled_up: bfloat16 [6144, 12288], P('grp', 'fs'), parts along dimension 0
- sampled_down: bfloat16 [24576, 3072], P(('grp', 'fs')), parts along dimension 0
The draws below stay inside these ranges and needn't reach their ends.
There are 2 independent parts, one for each index of `grp`. The reference program is written for one: setup_inputs(seed, part) draws one part's arguments, and reference() takes and returns one part's arrays. A program takes and returns all parts, laid end to end along the dimension named above; an argument that names none is the same for every part. Nothing has to cross between parts.
All inputs are finite; a program needn't handle non-finite values.
Results may differ from the reference program's by a relative error of at most 0.0074.
Values may be sent and summed in bfloat16 or wider, within the bound.
A program may use at most 192 MiB of HBM per device.

```python
import jax
import jax.numpy as jnp
from jax import lax

D = 3072
FF = 12288
TOKENS = 1024


def block_levels(own_key, shape, split, low, high):
    level = 1.0
    for position, parts in split:
        steps = jax.random.uniform(jax.random.fold_in(jax.random.fold_in(own_key, 6), position), (parts,), jnp.float32, low / len(split), high / len(split))
        level = level * jnp.repeat(jnp.exp(steps), shape[position] // parts).reshape((-1,) + (1,) * (len(shape) - 1 - position))
    return level


def normal_values(key, shape, scale, limit, split=(), held_as=jnp.bfloat16):
    factor_of = block_levels(key, shape, split, -0.22, 0.18) if split else 1.0
    array = jax.random.normal(key, shape, jnp.float32) * scale * factor_of
    return jnp.minimum(jnp.maximum(array, -limit), limit).astype(held_as)


def setup_inputs(seed: int = 0, part: int = 0) -> dict:
    keys = jax.random.split(jax.random.key(seed), 5)
    own_keys = jax.random.split(jax.random.fold_in(keys[4], part), 5)
    return {
        "tokens": normal_values(own_keys[0], (TOKENS, D), 1.0, 6.0, ((0, 4),)),
        "up_master": normal_values(keys[1], (D, FF), D ** -0.5, 0.109375, ((0, 4), (1, 4)), jnp.float32),
        "down_master": normal_values(keys[2], (FF, D), FF ** -0.5, 0.0546875, ((0, 4), (1, 4)), jnp.float32),
        "norm_gain": jnp.clip(1.0 + 0.18 * jax.random.normal(keys[3], (D,), jnp.float32), 0.1, 1.9),
    }


def reference(tokens, up_master, down_master, norm_gain):
    sampled_up = (norm_gain[:, None] * up_master).astype(jnp.bfloat16)
    sampled_down = down_master.astype(jnp.bfloat16)
    values = tokens.astype(jnp.float32)
    center = lax.optimization_barrier(jnp.mean(values, axis=-1, keepdims=True))
    spread = lax.optimization_barrier(jnp.mean(jnp.square(values - center), axis=-1, keepdims=True))
    normalized = ((values - center) * lax.rsqrt(spread + 1e-05)).astype(jnp.bfloat16)
    before = jnp.dot(normalized, sampled_up, preferred_element_type=jnp.float32)
    hidden = jnp.square(jax.nn.relu(before)).astype(jnp.bfloat16)
    prompt_out = jnp.dot(hidden, sampled_down, preferred_element_type=jnp.float32).astype(jnp.bfloat16)
    return (prompt_out, sampled_up, sampled_down)
```

```python
import functools

import jax
import jax.numpy as jnp
from jax import lax
from jax.experimental import pallas as pl
from jax.experimental.pallas import tpu as pltpu
from jax.sharding import PartitionSpec as P

MESH = pl.DeviceIdType.MESH
CORES = 2
PLANES = 2
LAG = 3
UNIT = 256
LINE = 16
LIMIT = 24
UP_CUTS = 6
DOWN_CUTS = 6
SHARED = 8
SHARES = 16


def normalize(tokens):
    values = tokens.astype(jnp.float32)
    center = jnp.mean(values, axis=-1, keepdims=True)
    spread = jnp.mean(jnp.square(values - center), axis=-1, keepdims=True)
    return ((values - center) * lax.rsqrt(spread + 1e-05)).astype(jnp.bfloat16)


def pieces_of(size, unit, most):
    for count in range(most, 1, -1):
        if size % (count * unit) == 0:
            return count
    return 1


def shared_rows(height):
    return height * SHARED // SHARES // (2 * LINE) * (2 * LINE)


def up_order(fs, cuts):
    events = []
    for cut in range(cuts):
        at = (cut + 1) / cuts
        events.append((at, 0, "relay", 0, cut))
        for j in range(fs):
            pace = (1.0, 1.25, 2.0, 2.0)[j]
            events.append((at * pace, 1 + j, "arrive", j, cut))
    events.append((0.55, 9, "split", 0, 0))
    events.append((0.85, 9, "shared", 0, 0))
    return [event[2:] for event in sorted(events)]


def hand_over(dims, cuts, tokens_ref, gain_ref, up_ref, master_ref, got_up, got_down, out_ref, rows_ref, gains, up_stage, up_src, relayed, stage, hidden, keep, send1, recv1, send2, recv2, up_sems, down_sems, sum_sems, load_sems):
    groups, fs, tp = dims
    up_cuts, down_cuts = cuts
    y, f, t = lax.axis_index("grp"), lax.axis_index("fs"), lax.axis_index("tp")
    x, k = t // CORES, t % CORES
    home_send, cross_send, first_recv, relay_send, relay_recv, y_send, y_recv, a_send, a_recv, b_send, b_recv = up_sems
    own_send, own_recv, split_send, split_recv, shared_send, shared_recv, dy_send, dy_recv, da_send, da_recv, ds_send, ds_recv, db_send, db_recv = down_sems
    send1_send, send1_recv, send2_send, send2_recv = sum_sems
    load_up, load_down, load_tokens = load_sems
    rows, cols = up_src.shape[1], up_src.shape[2] // up_cuts
    depth = got_up.shape[0] * got_up.shape[1] * got_up.shape[2]
    height, width = master_ref.shape
    tile = width // down_cuts
    both = shared_rows(height)
    part = (height - both) // groups
    near = f + 1 - 2 * (f % 2)
    rows_from = (f, near, (f + 2) % fs, (near + 2) % fs)
    sibling = (y, f, x * CORES + (1 - k))
    across_y = (1 - y, f, t)
    other = (1 - x) * CORES
    across_x = (y, f, other + k)

    def remote(src, dst, send, recv, where):
        return pltpu.make_async_remote_copy(src_ref=src, dst_ref=dst, send_sem=send, recv_sem=recv, device_id=where, device_id_type=MESH)

    def up_at(ref, group, lane, cut):
        return ref.at[group * CORES + lane, :, pl.ds(cut * cols, cols)]

    def src_at(lane, cut):
        return up_src.at[lane, :, pl.ds(cut * cols, cols)]

    def up_load(lane, cut):
        at = pl.ds(cut * cols, cols)
        return pltpu.make_async_copy(up_ref.at[y * CORES + lane, :, at], up_stage.at[lane, :, at], load_up.at[lane, cut])

    def up_local(cut):
        return pltpu.make_async_copy(src_at(k, cut), up_at(got_up.at[f], y, k, cut), first_recv.at[f, cut])

    def up_home(lane, cut):
        return remote(src_at(lane, cut), up_at(got_up.at[f], y, lane, cut), home_send.at[lane, cut], first_recv.at[f, cut], (y, t, x * CORES + lane))

    def up_cross_own(lane, cut):
        return remote(src_at(lane, cut), up_at(got_up.at[f], y, lane, cut), cross_send.at[lane, cut], first_recv.at[f, cut], (y, f, other + lane))

    def up_cross(lane, cut):
        return remote(src_at(lane, cut), relayed.at[k, :, pl.ds(cut * cols, cols)], cross_send.at[lane, cut], relay_recv.at[k, cut], (y, f, other + lane))

    def up_relay(slot, cut):
        return remote(relayed.at[slot, :, pl.ds(cut * cols, cols)], up_at(got_up.at[f], y, k, cut), relay_send.at[slot, cut], first_recv.at[f, cut], (y, other + slot, t))

    def up_here(r, cut):
        return pltpu.make_async_copy(src_at(0, cut), up_at(got_up.at[r], y, k, cut), first_recv.at[r, cut])

    def relay_here(slot, cut):
        return pltpu.make_async_copy(src_at(0, cut), relayed.at[slot, :, pl.ds(cut * cols, cols)], relay_recv.at[slot, cut])

    def up_y(r, cut):
        here = up_at(got_up.at[r], y, k, cut)
        return remote(here, here, y_send.at[r, cut], y_recv.at[r, cut], across_y)

    def up_a(r, cut):
        here = up_at(got_up.at[r], y, k, cut)
        return remote(here, here, a_send.at[r, cut], a_recv.at[r, cut], sibling)

    def up_b(r, cut):
        here = up_at(got_up.at[r], 1 - y, k, cut)
        return remote(here, here, b_send.at[r, cut], b_recv.at[r, cut], sibling)

    def tile_at(first, size, column, cut):
        return got_down.at[pl.ds(pl.multiple_of(first, LINE), size), pl.ds(pl.multiple_of(column * width + cut * tile, tile), tile)]

    def split_at(group, column, cut):
        return tile_at(group * part, part, column, cut)

    def shared_at(column, cut):
        return tile_at(groups * part, both, column, cut)

    def down_split(cut):
        here = split_at(y, t, cut)
        return remote(here, here, split_send.at[cut], split_recv.at[cut], across_x)

    def down_shared(cut):
        here = shared_at(t, cut)
        return remote(here, here, shared_send.at[cut], shared_recv.at[cut], across_x)

    def down_y(cut):
        here = split_at(y, other + k, cut)
        return remote(here, here, dy_send.at[cut], dy_recv.at[cut], across_y)

    def down_a(cut):
        here = split_at(y, other + k, cut)
        return remote(here, here, da_send.at[cut], da_recv.at[cut], sibling)

    def down_s(cut):
        here = shared_at(other + k, cut)
        return remote(here, here, ds_send.at[cut], ds_recv.at[cut], sibling)

    def down_b(cut):
        here = split_at(1 - y, other + k, cut)
        return remote(here, here, db_send.at[cut], db_recv.at[cut], sibling)

    own_columns = got_down.at[:, pl.ds(pl.multiple_of(t * width, width), width)]
    down_own = remote(own_columns, own_columns, own_send, own_recv, sibling)

    slab = stage.shape[1]
    slots = stage.shape[0]
    slabs = height // slab

    def take(step):
        return pltpu.make_async_copy(master_ref.at[pl.ds(step * slab, slab), :], stage.at[step % slots], load_down.at[step % slots])

    take_tokens = pltpu.make_async_copy(tokens_ref, rows_ref, load_tokens)

    for cut in range(up_cuts):
        for lane in range(CORES):
            up_load(lane, cut).start()
    for step in range(slots):
        take(step).start()
    take_tokens.start()

    barrier = pltpu.get_barrier_semaphore()
    partners = [sibling, across_y] + [(y, f, other + lane) for lane in range(CORES)]
    partners += [(y, rows_from[j], x * CORES + lane) for j in range(1, fs) for lane in range(CORES)]
    for partner in partners:
        pl.semaphore_signal(barrier, inc=1, device_id=partner, device_id_type=MESH)

    gains[...] = jnp.transpose(jnp.broadcast_to(gain_ref[...], (128, gain_ref.shape[1])))

    def up_cast(cut):
        for lane in range(CORES):
            up_load(lane, cut).wait()

            @pl.loop(0, rows // LINE)
            def _(line):
                at = pl.ds(pl.multiple_of(line * LINE, LINE), LINE)
                scale = gains[pl.ds(pl.multiple_of((y * CORES + lane) * rows + line * LINE, LINE), LINE), :]
                block = up_stage[lane, at, pl.ds(cut * cols, cols)]
                up_src[lane, at, pl.ds(cut * cols, cols)] = (jnp.concatenate([scale] * (cols // 128), axis=1) * block).astype(jnp.bfloat16)

    def up_start(cut):
        for lane in range(CORES):
            @pl.when(t == f)
            def _():
                up_cross_own(lane, cut).start()

            @pl.when(t != f)
            def _():
                up_cross(lane, cut).start()

        for lane in range(CORES):
            @pl.when(jnp.logical_or(t != f, lane != k))
            def _():
                up_home(lane, cut).start()

        @pl.when(t == f)
        def _():
            up_local(cut).start()

    up_cast(0)
    pl.semaphore_wait(barrier, len(partners))
    for cut in range(up_cuts):
        up_start(cut)
        if cut + 1 < up_cuts:
            up_cast(cut + 1)

    for step in range(slabs):
        take(step).wait()

        @pl.loop(0, slab // LINE)
        def _(line):
            start = pl.multiple_of(line * LINE, LINE)
            to = pl.ds(pl.multiple_of(step * slab + start, LINE), LINE)
            got_down[to, pl.ds(pl.multiple_of(t * width, width), width)] = stage[step % slots, pl.ds(start, LINE), :].astype(jnp.bfloat16)

        if step + slots < slabs:
            take(step + slots).start()
    down_own.start()

    take_tokens.wait()

    @pl.loop(0, tokens_ref.shape[0] // LINE)
    def _(step):
        at = pl.ds(pl.multiple_of(step * LINE, LINE), LINE)
        rows_ref[at, :] = normalize(rows_ref[at, :])

    def hidden_units(cut):
        @pl.loop(0, cols // UNIT)
        def _(step):
            at = pl.ds(pl.multiple_of(cut * cols + step * UNIT, UNIT), UNIT)
            block = got_up[:, :, :, at].reshape(depth, UNIT)
            before = jnp.dot(rows_ref[...], block, preferred_element_type=jnp.float32)
            hidden[:, at] = jnp.square(jnp.maximum(before, 0.0)).astype(jnp.bfloat16)

    def up_arrive(j, cut):
        r = rows_from[j]
        up_here(r, cut).wait()
        up_y(r, cut).start()
        up_a(r, cut).start()

    def up_second(j, cut):
        r = rows_from[j]
        up_y(r, cut).wait_recv()
        up_b(r, cut).start()

    def up_done(cut):
        for j in range(fs):
            up_a(rows_from[j], cut).wait_recv()
            up_b(rows_from[j], cut).wait_recv()
        hidden_units(cut)

    waiting, seen, ready = [], [0] * up_cuts, []

    def follow():
        j, cut = waiting.pop(0)
        up_second(j, cut)
        seen[cut] += 1
        if seen[cut] == fs:
            ready.append(cut)

    for kind, j, cut in up_order(fs, up_cuts):
        if kind == "relay":
            for slot in range(CORES):
                @pl.when(other + slot != f)
                def _():
                    relay_here(slot, cut).wait()
                    up_relay(slot, cut).start()
        elif kind == "split":
            for piece in range(down_cuts):
                down_split(piece).start()
        elif kind == "shared":
            for piece in range(down_cuts):
                down_shared(piece).start()
        else:
            up_arrive(j, cut)
            waiting.append((j, cut))
            if len(waiting) > LAG:
                follow()
            elif len(ready) > 1:
                up_done(ready.pop(0))

    for cut in range(down_cuts):
        down_split(cut).wait_recv()
        down_y(cut).start()
        down_a(cut).start()
    while waiting:
        follow()
    while ready:
        up_done(ready.pop(0))

    def sum_near(g, cut):
        at = pl.ds(cut * tile, tile)
        return remote(send1.at[g, :, at], recv1.at[g, :, at], send1_send.at[g, cut], send1_recv.at[g, cut], (y, near, t))

    def sum_far(cut):
        at = pl.ds(cut * tile, tile)
        return remote(send2.at[:, at], recv2.at[:, at], send2_send.at[cut], send2_recv.at[cut], (y, rows_from[2], t))

    bases = (x * CORES, other)
    close = (x == f // CORES, x != f // CORES)

    def term(column, cut):
        at = pl.ds(pl.multiple_of(column * width + cut * tile, tile), tile)
        return jnp.dot(hidden[...], got_down[:, at], preferred_element_type=jnp.float32)

    def features(g, cut):
        at = pl.ds(cut * tile, tile)
        send1[g, :, at] = term(bases[g] + 1 - f % 2, cut).astype(jnp.bfloat16)
        sum_near(g, cut).start()
        keep[g, :, at] = term(bases[g] + f % 2, cut)

    def merge(g, cut):
        at = pl.ds(cut * tile, tile)
        sum_near(g, cut).wait_recv()
        total = keep[g, :, at] + recv1[g, :, at].astype(jnp.float32)

        @pl.when(close[g])
        def _():
            keep[g, :, at] = total

        @pl.when(jnp.logical_not(close[g]))
        def _():
            send2[:, at] = total.astype(jnp.bfloat16)
            sum_far(cut).start()

    def finish(cut):
        at = pl.ds(cut * tile, tile)
        sum_far(cut).wait_recv()
        total = keep[(x + f // CORES) % PLANES, :, at] + recv2[:, at].astype(jnp.float32)
        out_ref[:, at] = total.astype(jnp.bfloat16)

    down_own.wait_recv()
    for step in range(down_cuts + 3):
        if step < down_cuts:
            features(0, step)
            down_shared(step).wait_recv()
            down_s(step).start()
            down_y(step).wait_recv()
            down_b(step).start()
        if 1 <= step <= down_cuts:
            cut = step - 1
            down_a(cut).wait_recv()
            down_s(cut).wait_recv()
            down_b(cut).wait_recv()
            features(1, cut)
            merge(0, cut)
        if 2 <= step <= down_cuts + 1:
            merge(1, step - 2)
        if step >= 3:
            finish(step - 3)

    for cut in range(up_cuts):
        for lane in range(CORES):
            up_cross(lane, cut).wait_send()

            @pl.when(jnp.logical_or(t != f, lane != k))
            def _():
                up_home(lane, cut).wait_send()

        for slot in range(CORES):
            @pl.when(other + slot != f)
            def _():
                up_relay(slot, cut).wait_send()
        for j in range(fs):
            up_y(rows_from[j], cut).wait_send()
            up_a(rows_from[j], cut).wait_send()
            up_b(rows_from[j], cut).wait_send()
    down_own.wait_send()
    for cut in range(down_cuts):
        down_split(cut).wait_send()
        down_shared(cut).wait_send()
        down_y(cut).wait_send()
        down_a(cut).wait_send()
        down_s(cut).wait_send()
        down_b(cut).wait_send()
        sum_near(0, cut).wait_send()
        sum_near(1, cut).wait_send()
        sum_far(cut).wait_send()


def fused(tokens_in, up_master, down_master, norm_gain, dims):
    groups, fs, tp = dims
    rows, cols = up_master.shape[0] // (groups * CORES), up_master.shape[1]
    height, width = down_master.shape
    tokens = tokens_in.shape[0]
    up_cuts = pieces_of(cols, UNIT, UP_CUTS)
    down_cuts = pieces_of(width, 128, DOWN_CUTS)
    slabs = pieces_of(height, LINE, 8)
    dma = pltpu.SemaphoreType.DMA
    lanes, whole, strip = dma((CORES, up_cuts)), dma((fs, up_cuts)), dma((down_cuts,))
    up_sems = [lanes, lanes, whole, lanes, lanes] + [whole] * 6
    down_sems = [dma, dma] + [strip] * 12
    sum_sems = [dma((2, down_cuts)), dma((2, down_cuts)), strip, strip]
    vmem = pl.BlockSpec(memory_space=pltpu.VMEM)
    hbm = pl.BlockSpec(memory_space=pl.ANY)
    got_up, got_down, out = pl.pallas_call(
        functools.partial(hand_over, dims, (up_cuts, down_cuts)),
        out_shape=(
            pltpu.VMEM((fs, groups * CORES, rows, cols), jnp.bfloat16),
            pltpu.VMEM((height, tp * width), jnp.bfloat16),
            jax.ShapeDtypeStruct((tokens, width), jnp.bfloat16),
        ),
        in_specs=[hbm, vmem, hbm, hbm],
        out_specs=(vmem, vmem, vmem),
        scratch_shapes=[
            pltpu.VMEM(tokens_in.shape, jnp.bfloat16),
            pltpu.VMEM((up_master.shape[0], 128), jnp.float32),
            pltpu.VMEM((CORES, rows, cols), jnp.float32),
            pltpu.VMEM((CORES, rows, cols), jnp.bfloat16),
            pltpu.VMEM((CORES, rows, cols), jnp.bfloat16),
            pltpu.VMEM((2, height // slabs, width), jnp.float32),
            pltpu.VMEM((tokens, cols), jnp.bfloat16),
            pltpu.VMEM((2, tokens, width), jnp.float32),
            pltpu.VMEM((2, tokens, width), jnp.bfloat16),
            pltpu.VMEM((2, tokens, width), jnp.bfloat16),
            pltpu.VMEM((tokens, width), jnp.bfloat16),
            pltpu.VMEM((tokens, width), jnp.bfloat16),
            up_sems,
            down_sems,
            sum_sems,
            [lanes, dma((2,)), dma],
        ],
        compiler_params=pltpu.CompilerParams(collective_id=0, has_side_effects=True, vmem_limit_bytes=LIMIT << 20),
    )(tokens_in, norm_gain.reshape(1, -1), up_master.reshape(groups * CORES, rows, cols), down_master)
    return out, got_up.reshape(fs * groups * CORES * rows, cols), got_down


def fits(up_shape, down_shape, dims):
    groups, fs, tp = dims
    own = 2 * (up_shape[0] * up_shape[1] * fs + down_shape[0] * down_shape[1] * tp)
    aligned = up_shape[0] % (groups * CORES * LINE) == 0 and up_shape[0] % 128 == 0 and up_shape[1] % UNIT == 0
    square = groups == 2 and tp == CORES * PLANES and fs == tp
    return square and aligned and down_shape[0] % (groups * LINE) == 0 and down_shape[1] % 128 == 0 and own <= 40 << 20


def by_collectives(normalized, up_cast, down_cast):
    quarter = lax.all_to_all(up_cast, "tp", split_axis=0, concat_axis=1, tiled=True)
    moved = lax.all_to_all(quarter, "fs", split_axis=1, concat_axis=0, tiled=True)
    part_rows = quarter.shape[0]
    stacked = moved.reshape(moved.shape[0] // part_rows, part_rows, moved.shape[1])
    joined = lax.all_gather(stacked, "tp", axis=1, tiled=True)
    sampled_down = lax.all_gather(down_cast, "tp", axis=1, tiled=True)
    sampled_up = joined.reshape(joined.shape[0] * joined.shape[1], joined.shape[2])
    before = jnp.dot(normalized, sampled_up, preferred_element_type=jnp.float32)
    hidden = jnp.square(jax.nn.relu(before)).astype(jnp.bfloat16)
    terms = jnp.dot(hidden, sampled_down, preferred_element_type=jnp.float32)
    summed = lax.psum_scatter(terms, "fs", scatter_dimension=1, tiled=True)
    return summed.astype(jnp.bfloat16), sampled_up, sampled_down


def shards(dims, tokens, up_master, down_master, norm_gain):
    if fits(up_master.shape, down_master.shape, dims):
        return fused(tokens, up_master, down_master, norm_gain, dims)
    up_cast = (norm_gain[:, None] * up_master).astype(jnp.bfloat16)
    return by_collectives(normalize(tokens), up_cast, down_master.astype(jnp.bfloat16))


def solution(mesh):
    dims = tuple(mesh.shape[name] for name in ("grp", "fs", "tp"))
    return jax.shard_map(
        functools.partial(shards, dims),
        mesh=mesh,
        in_specs=(P(("grp", "tp"), None), P("fs", "tp"), P("fs", "tp"), P("fs")),
        out_specs=(P(("grp", "tp"), "fs"), P("grp", "fs"), P(("grp", "fs"), None)),
        check_vma=False,
    )
```

```python
import functools

import jax
import jax.numpy as jnp
from jax import lax
from jax.experimental import pallas as pl
from jax.experimental.pallas import tpu as pltpu
from jax.sharding import PartitionSpec as P

MESH = pl.DeviceIdType.MESH
CORES = 2
PLANES = 2
LAG = 3
UNIT = 256
LINE = 16
LIMIT = 24
START = 0.15
UP_CUTS = 6
DOWN_CUTS = 6
SHARED = 9
SHARES = 16


def normalize(tokens):
    values = tokens.astype(jnp.float32)
    center = jnp.mean(values, axis=-1, keepdims=True)
    spread = jnp.mean(jnp.square(values - center), axis=-1, keepdims=True)
    return ((values - center) * lax.rsqrt(spread + 1e-05)).astype(jnp.bfloat16)


def pieces_of(size, unit, most):
    for count in range(most, 1, -1):
        if size % (count * unit) == 0:
            return count
    return 1


def shared_rows(height):
    return height * SHARED // SHARES // (2 * LINE) * (2 * LINE)


def order_of(fs, up_cuts, down_cuts, share):
    ready = []
    for cut in range(up_cuts):
        at = (cut + 1) / up_cuts
        ready.append((START + at, 0, "relay", 0, cut))
        for j, came in enumerate((START + at, START + 0.1 + 1.5 * at, START + 0.2 + 1.5 * at, START + 1.15 + at)):
            ready.append((came, 1, "arrive", j, cut))
    for cut in range(down_cuts):
        at = (cut + 1) / down_cuts
        ready.append((START + 1.05 + (1 - share) * at, 2, "split", 0, cut))
        ready.append((START + 1.05 + 1 - share + 2 * share * at, 4, "shared", 0, cut))
    ready.append((START + 0.3, 0, "send", 0, 0))
    ready.append((START + 0.6, 0, "send", 1, 0))
    ready.sort()
    order, spare, now = [], [], START
    for came, _, kind, j, cut in ready:
        while spare and kind == "arrive" and now + (1 - share) / down_cuts <= came:
            order.append(("cross", 0, spare.pop(0)))
            now += (1 - share) / down_cuts
        order.append((kind, j, cut))
        if kind == "arrive":
            now = max(now, came) + 2 / (fs * up_cuts)
        if kind == "split":
            spare.append(cut)
    last = max(i for i, entry in enumerate(order) if entry[0] == "arrive") + 1
    return order[:last], spare


def hand_over(dims, cuts, tokens_ref, gain_ref, up_ref, master_ref, got_up, got_down, out_ref, rows_ref, gains, up_stage, up_src, relayed, stage, hidden, keep, send1, recv1, send2, recv2, up_sems, down_sems, sum_sems, load_sems):
    groups, fs, tp = dims
    up_cuts, down_cuts = cuts
    y, f, t = lax.axis_index("grp"), lax.axis_index("fs"), lax.axis_index("tp")
    x, k = t // CORES, t % CORES
    home_send, cross_send, first_recv, relay_send, relay_recv, y_send, y_recv, a_send, a_recv, b_send, b_recv = up_sems
    own_send, own_recv, split_send, split_recv, shared_send, shared_recv, dy_send, dy_recv, da_send, da_recv, ds_send, ds_recv, db_send, db_recv = down_sems
    send1_send, send1_recv, send2_send, send2_recv = sum_sems
    load_up, load_down, load_tokens = load_sems
    rows, cols = up_src.shape[1], up_src.shape[2] // up_cuts
    depth = got_up.shape[0] * got_up.shape[1] * got_up.shape[2]
    height, width = master_ref.shape
    tile = width // down_cuts
    both = shared_rows(height)
    part = (height - both) // groups
    near = f + 1 - 2 * (f % 2)
    rows_from = (f, near, (fs - 1) * (1 - f // 2), 2 - f // 2)
    facing = (f + 2) % fs
    sibling = (y, f, x * CORES + (1 - k))
    across_y = (1 - y, f, t)
    other = (1 - x) * CORES
    across_x = (y, f, other + k)

    def remote(src, dst, send, recv, where):
        return pltpu.make_async_remote_copy(src_ref=src, dst_ref=dst, send_sem=send, recv_sem=recv, device_id=where, device_id_type=MESH)

    def up_at(ref, group, lane, cut):
        return ref.at[group * CORES + lane, :, pl.ds(cut * cols, cols)]

    def src_at(lane, cut):
        return up_src.at[lane, :, pl.ds(cut * cols, cols)]

    def up_load(lane, cut):
        at = pl.ds(cut * cols, cols)
        return pltpu.make_async_copy(up_ref.at[y * CORES + lane, :, at], up_stage.at[lane, :, at], load_up.at[lane, cut])

    def up_local(cut):
        return pltpu.make_async_copy(src_at(k, cut), up_at(got_up.at[f], y, k, cut), first_recv.at[f, cut])

    def up_home(lane, cut):
        return remote(src_at(lane, cut), up_at(got_up.at[f], y, lane, cut), home_send.at[lane, cut], first_recv.at[f, cut], (y, t, x * CORES + lane))

    def up_cross_own(lane, cut):
        return remote(src_at(lane, cut), up_at(got_up.at[f], y, lane, cut), cross_send.at[lane, cut], first_recv.at[f, cut], (y, f, other + lane))

    def up_cross(lane, cut):
        return remote(src_at(lane, cut), relayed.at[k, :, pl.ds(cut * cols, cols)], cross_send.at[lane, cut], relay_recv.at[k, cut], (y, f, other + lane))

    def up_relay(slot, cut):
        return remote(relayed.at[slot, :, pl.ds(cut * cols, cols)], up_at(got_up.at[f], y, k, cut), relay_send.at[slot, cut], first_recv.at[f, cut], (y, other + slot, t))

    def up_here(r, cut):
        return pltpu.make_async_copy(src_at(0, cut), up_at(got_up.at[r], y, k, cut), first_recv.at[r, cut])

    def relay_here(slot, cut):
        return pltpu.make_async_copy(src_at(0, cut), relayed.at[slot, :, pl.ds(cut * cols, cols)], relay_recv.at[slot, cut])

    def up_y(r, cut):
        here = up_at(got_up.at[r], y, k, cut)
        return remote(here, here, y_send.at[r, cut], y_recv.at[r, cut], across_y)

    def up_a(r, cut):
        here = up_at(got_up.at[r], y, k, cut)
        return remote(here, here, a_send.at[r, cut], a_recv.at[r, cut], sibling)

    def up_b(r, cut):
        here = up_at(got_up.at[r], 1 - y, k, cut)
        return remote(here, here, b_send.at[r, cut], b_recv.at[r, cut], sibling)

    def tile_at(first, size, column, cut):
        return got_down.at[pl.ds(pl.multiple_of(first, LINE), size), pl.ds(pl.multiple_of(column * width + cut * tile, tile), tile)]

    def split_at(group, column, cut):
        return tile_at(group * part, part, column, cut)

    def shared_at(column, cut):
        return tile_at(groups * part, both, column, cut)

    def down_split(cut):
        here = split_at(y, t, cut)
        return remote(here, here, split_send.at[cut], split_recv.at[cut], across_x)

    def down_shared(cut):
        here = shared_at(t, cut)
        return remote(here, here, shared_send.at[cut], shared_recv.at[cut], across_x)

    def down_y(cut):
        here = split_at(y, other + k, cut)
        return remote(here, here, dy_send.at[cut], dy_recv.at[cut], across_y)

    def down_a(cut):
        here = split_at(y, other + k, cut)
        return remote(here, here, da_send.at[cut], da_recv.at[cut], sibling)

    def down_s(cut):
        here = shared_at(other + k, cut)
        return remote(here, here, ds_send.at[cut], ds_recv.at[cut], sibling)

    def down_b(cut):
        here = split_at(1 - y, other + k, cut)
        return remote(here, here, db_send.at[cut], db_recv.at[cut], sibling)

    own_columns = got_down.at[:, pl.ds(pl.multiple_of(t * width, width), width)]
    down_own = remote(own_columns, own_columns, own_send, own_recv, sibling)

    slab = stage.shape[1]
    slots = stage.shape[0]
    slabs = height // slab

    def take(step):
        return pltpu.make_async_copy(master_ref.at[pl.ds(step * slab, slab), :], stage.at[step % slots], load_down.at[step % slots])

    take_tokens = pltpu.make_async_copy(tokens_ref, rows_ref, load_tokens)

    for cut in range(up_cuts):
        for lane in range(CORES):
            up_load(lane, cut).start()
    for step in range(slots):
        take(step).start()
    take_tokens.start()

    barrier = pltpu.get_barrier_semaphore()
    partners = [sibling, across_y] + [(y, f, other + lane) for lane in range(CORES)]
    partners += [(y, rows_from[j], x * CORES + lane) for j in range(1, fs) for lane in range(CORES)]
    for partner in partners:
        pl.semaphore_signal(barrier, inc=1, device_id=partner, device_id_type=MESH)

    gains[...] = jnp.transpose(jnp.broadcast_to(gain_ref[...][None, :], (128, gain_ref.shape[0])))

    def up_cast(cut):
        for lane in range(CORES):
            up_load(lane, cut).wait()

            @pl.loop(0, rows // LINE)
            def _(line):
                at = pl.ds(pl.multiple_of(line * LINE, LINE), LINE)
                scale = gains[pl.ds(pl.multiple_of((y * CORES + lane) * rows + line * LINE, LINE), LINE), :]
                block = up_stage[lane, at, pl.ds(cut * cols, cols)]
                up_src[lane, at, pl.ds(cut * cols, cols)] = (jnp.concatenate([scale] * (cols // 128), axis=1) * block).astype(jnp.bfloat16)

    def up_start(cut):
        for lane in range(CORES):
            @pl.when(t == f)
            def _():
                up_cross_own(lane, cut).start()

            @pl.when(t != f)
            def _():
                up_cross(lane, cut).start()

    def up_direct(cut):
        for lane in range(CORES):
            @pl.when(jnp.logical_or(t != f, lane != k))
            def _():
                up_home(lane, cut).start()

        @pl.when(t == f)
        def _():
            up_local(cut).start()

    for cut in range(up_cuts):
        up_cast(cut)
    pl.semaphore_wait(barrier, len(partners))
    for cut in range(up_cuts):
        up_start(cut)
        if cut == 0:
            up_direct(cut)

    for step in range(slabs):
        take(step).wait()

        @pl.loop(0, slab // LINE)
        def _(line):
            start = pl.multiple_of(line * LINE, LINE)
            to = pl.ds(pl.multiple_of(step * slab + start, LINE), LINE)
            got_down[to, pl.ds(pl.multiple_of(t * width, width), width)] = stage[step % slots, pl.ds(start, LINE), :].astype(jnp.bfloat16)

        if step + slots < slabs:
            take(step + slots).start()
    down_own.start()

    take_tokens.wait()

    @pl.loop(0, tokens_ref.shape[0] // LINE)
    def _(step):
        at = pl.ds(pl.multiple_of(step * LINE, LINE), LINE)
        rows_ref[at, :] = normalize(rows_ref[at, :])

    def hidden_units(cut):
        @pl.loop(0, cols // UNIT)
        def _(step):
            at = pl.ds(pl.multiple_of(cut * cols + step * UNIT, UNIT), UNIT)
            block = got_up[:, :, :, at].reshape(depth, UNIT)
            before = jnp.dot(rows_ref[...], block, preferred_element_type=jnp.float32)
            hidden[:, at] = jnp.square(jnp.maximum(before, 0.0)).astype(jnp.bfloat16)

    def up_arrive(j, cut):
        r = rows_from[j]
        up_here(r, cut).wait()
        up_y(r, cut).start()
        up_a(r, cut).start()

    def up_second(j, cut):
        r = rows_from[j]
        up_y(r, cut).wait_recv()
        up_b(r, cut).start()

    def up_done(cut):
        for j in range(fs):
            up_a(rows_from[j], cut).wait_recv()
            up_b(rows_from[j], cut).wait_recv()
        hidden_units(cut)

    def sum_near(g, cut):
        at = pl.ds(cut * tile, tile)
        return remote(send1.at[g, :, at], recv1.at[g, :, at], send1_send.at[g, cut], send1_recv.at[g, cut], (y, near, t))

    def sum_far(cut):
        at = pl.ds(cut * tile, tile)
        return remote(send2.at[:, at], recv2.at[:, at], send2_send.at[cut], send2_recv.at[cut], (y, facing, t))

    bases = (x * CORES, other)
    close = (x == f // CORES, x != f // CORES)

    def features(g, cut):
        at = pl.ds(cut * tile, tile)
        other_at, here_at = (pl.ds(pl.multiple_of(column * width + cut * tile, tile), tile) for column in (bases[g] + 1 - f % 2, bases[g] + f % 2))
        both_terms = jnp.zeros((hidden.shape[0], 2 * tile), jnp.float32)
        for unit in range(0, height, UNIT):
            rows_at = pl.ds(unit, UNIT)
            block = jnp.concatenate([got_down[rows_at, other_at], got_down[rows_at, here_at]], axis=1)
            both_terms += jnp.dot(hidden[:, rows_at], block, preferred_element_type=jnp.float32)
        send1[g, :, at] = both_terms[:, :tile].astype(jnp.bfloat16)
        sum_near(g, cut).start()
        keep[g, :, at] = both_terms[:, tile:]

    def merge(g, cut):
        at = pl.ds(cut * tile, tile)
        sum_near(g, cut).wait_recv()
        total = keep[g, :, at] + recv1[g, :, at].astype(jnp.float32)

        @pl.when(close[g])
        def _():
            keep[g, :, at] = total

        @pl.when(jnp.logical_not(close[g]))
        def _():
            send2[:, at] = total.astype(jnp.bfloat16)
            sum_far(cut).start()

    def finish(cut):
        at = pl.ds(cut * tile, tile)
        sum_far(cut).wait_recv()
        total = keep[(x + f // CORES) % PLANES, :, at] + recv2[:, at].astype(jnp.float32)
        out_ref[:, at] = total.astype(jnp.bfloat16)

    waiting, seen, ready, crossed, shared = [], [0] * up_cuts, [], [], []

    def follow():
        kind, j, cut = waiting.pop(0)
        if kind == "cross":
            down_y(cut).wait_recv()
            down_b(cut).start()
            crossed.append(cut)
        else:
            up_second(j, cut)
            seen[cut] += 1
            if seen[cut] == fs:
                ready.append(cut)

    def shared_in(cut):
        down_shared(cut).wait_recv()
        down_s(cut).start()
        shared.append(cut)

    order, late = order_of(fs, up_cuts, down_cuts, both / height)
    for kind, j, cut in order:
        if kind == "relay":
            for slot in range(CORES):
                @pl.when(other + slot != f)
                def _():
                    relay_here(slot, cut).wait()
                    up_relay(slot, cut).start()

            if cut + 1 < up_cuts:
                up_direct(cut + 1)
        elif kind == "send":
            for piece in range(down_cuts):
                (down_split, down_shared)[j](piece).start()
        elif kind == "split":
            down_split(cut).wait_recv()
            down_a(cut).start()
        elif kind == "shared":
            shared_in(cut)
        else:
            if kind == "cross":
                down_y(cut).start()
            else:
                up_arrive(j, cut)
            waiting.append((kind, j, cut))
            if len(waiting) > LAG:
                follow()
            if len(ready) > 1:
                up_done(ready.pop(0))

    for cut in late:
        down_y(cut).start()
        waiting.append(("cross", 0, cut))
    while sum(seen) < fs * up_cuts:
        follow()
        while ready:
            up_done(ready.pop(0))
    down_own.wait_recv()

    merging, merged, paired = [], [0] * down_cuts, 0

    def settle(limit):
        while len(merging) > limit:
            g, cut = merging.pop(0)
            merge(g, cut)
            merged[cut] += 1

    for step in range(down_cuts):
        features(0, step)
        merging.append((0, step))
        if step % 2 == 1:
            if waiting:
                follow()
            settle(3)
    while paired < down_cuts:
        if len(shared) < down_cuts and len(shared) <= len(crossed):
            shared_in(len(shared))
        if waiting:
            follow()
        if paired + 1 < len(crossed) or not waiting:
            down_a(paired).wait_recv()
            down_s(paired).wait_recv()
            down_b(paired).wait_recv()
            features(1, paired)
            merging.append((1, paired))
            paired += 1
        settle(2)
    settle(0)
    for cut in range(down_cuts):
        finish(cut)

    for cut in range(up_cuts):
        for lane in range(CORES):
            up_cross(lane, cut).wait_send()

            @pl.when(jnp.logical_or(t != f, lane != k))
            def _():
                up_home(lane, cut).wait_send()

        for slot in range(CORES):
            @pl.when(other + slot != f)
            def _():
                up_relay(slot, cut).wait_send()
        for j in range(fs):
            up_y(rows_from[j], cut).wait_send()
            up_a(rows_from[j], cut).wait_send()
            up_b(rows_from[j], cut).wait_send()
    down_own.wait_send()
    for cut in range(down_cuts):
        down_split(cut).wait_send()
        down_shared(cut).wait_send()
        down_y(cut).wait_send()
        down_a(cut).wait_send()
        down_s(cut).wait_send()
        down_b(cut).wait_send()
        sum_near(0, cut).wait_send()
        sum_near(1, cut).wait_send()
        sum_far(cut).wait_send()


def fused(tokens_in, up_master, down_master, norm_gain, dims):
    groups, fs, tp = dims
    rows, cols = up_master.shape[0] // (groups * CORES), up_master.shape[1]
    height, width = down_master.shape
    tokens = tokens_in.shape[0]
    up_cuts = pieces_of(cols, UNIT, UP_CUTS)
    down_cuts = pieces_of(width, 128, DOWN_CUTS)
    slabs = pieces_of(height, LINE, 8)
    dma = pltpu.SemaphoreType.DMA
    lanes, whole, strip = dma((CORES, up_cuts)), dma((fs, up_cuts)), dma((down_cuts,))
    up_sems = [lanes, lanes, whole, lanes, lanes] + [whole] * 6
    down_sems = [dma, dma] + [strip] * 12
    sum_sems = [dma((2, down_cuts)), dma((2, down_cuts)), strip, strip]
    vmem = pl.BlockSpec(memory_space=pltpu.VMEM)
    hbm = pl.BlockSpec(memory_space=pl.ANY)
    got_up, got_down, out = pl.pallas_call(
        functools.partial(hand_over, dims, (up_cuts, down_cuts)),
        out_shape=(
            pltpu.VMEM((fs, groups * CORES, rows, cols), jnp.bfloat16),
            pltpu.VMEM((height, tp * width), jnp.bfloat16),
            jax.ShapeDtypeStruct((tokens, width), jnp.bfloat16),
        ),
        in_specs=[hbm, vmem, hbm, hbm],
        out_specs=(vmem, vmem, vmem),
        scratch_shapes=[
            pltpu.VMEM(tokens_in.shape, jnp.bfloat16),
            pltpu.VMEM((up_master.shape[0], 128), jnp.float32),
            pltpu.VMEM((CORES, rows, cols), jnp.float32),
            pltpu.VMEM((CORES, rows, cols), jnp.bfloat16),
            pltpu.VMEM((CORES, rows, cols), jnp.bfloat16),
            pltpu.VMEM((2, height // slabs, width), jnp.float32),
            pltpu.VMEM((tokens, cols), jnp.bfloat16),
            pltpu.VMEM((2, tokens, width), jnp.float32),
            pltpu.VMEM((2, tokens, width), jnp.bfloat16),
            pltpu.VMEM((2, tokens, width), jnp.bfloat16),
            pltpu.VMEM((tokens, width), jnp.bfloat16),
            pltpu.VMEM((tokens, width), jnp.bfloat16),
            up_sems,
            down_sems,
            sum_sems,
            [lanes, dma((2,)), dma],
        ],
        compiler_params=pltpu.CompilerParams(collective_id=0, has_side_effects=True, vmem_limit_bytes=LIMIT << 20),
    )(tokens_in, norm_gain, up_master.reshape(groups * CORES, rows, cols), down_master)
    return out, got_up.reshape(fs * groups * CORES * rows, cols), got_down


def fits(up_shape, down_shape, dims):
    groups, fs, tp = dims
    own = 2 * (up_shape[0] * up_shape[1] * fs + down_shape[0] * down_shape[1] * tp)
    aligned = up_shape[0] % (groups * CORES * LINE) == 0 and up_shape[0] % 128 == 0 and up_shape[1] % UNIT == 0
    square = groups == 2 and tp == CORES * PLANES and fs == tp
    return square and aligned and down_shape[0] % UNIT == 0 and down_shape[1] % 128 == 0 and own <= 40 << 20


def by_collectives(normalized, up_cast, down_cast):
    quarter = lax.all_to_all(up_cast, "tp", split_axis=0, concat_axis=1, tiled=True)
    moved = lax.all_to_all(quarter, "fs", split_axis=1, concat_axis=0, tiled=True)
    part_rows = quarter.shape[0]
    stacked = moved.reshape(moved.shape[0] // part_rows, part_rows, moved.shape[1])
    joined = lax.all_gather(stacked, "tp", axis=1, tiled=True)
    sampled_down = lax.all_gather(down_cast, "tp", axis=1, tiled=True)
    sampled_up = joined.reshape(joined.shape[0] * joined.shape[1], joined.shape[2])
    before = jnp.dot(normalized, sampled_up, preferred_element_type=jnp.float32)
    hidden = jnp.square(jax.nn.relu(before)).astype(jnp.bfloat16)
    terms = jnp.dot(hidden, sampled_down, preferred_element_type=jnp.float32)
    summed = lax.psum_scatter(terms, "fs", scatter_dimension=1, tiled=True)
    return summed.astype(jnp.bfloat16), sampled_up, sampled_down


def shards(dims, tokens, up_master, down_master, norm_gain):
    if fits(up_master.shape, down_master.shape, dims):
        return fused(tokens, up_master, down_master, norm_gain, dims)
    up_cast = (norm_gain[:, None] * up_master).astype(jnp.bfloat16)
    return by_collectives(normalize(tokens), up_cast, down_master.astype(jnp.bfloat16))


def solution(mesh):
    dims = tuple(mesh.shape[name] for name in ("grp", "fs", "tp"))
    return jax.shard_map(
        functools.partial(shards, dims),
        mesh=mesh,
        in_specs=(P(("grp", "tp"), None), P("fs", "tp"), P("fs", "tp"), P("fs")),
        out_specs=(P(("grp", "tp"), "fs"), P("grp", "fs"), P(("grp", "fs"), None)),
        check_vma=False,
    )
```

```python
import functools

import jax
import jax.numpy as jnp
from jax import lax
from jax.experimental import pallas as pl
from jax.experimental.pallas import tpu as pltpu
from jax.sharding import PartitionSpec as P

MESH = pl.DeviceIdType.MESH
CORES = 2
PLANES = 2
LAG = 3
UNIT = 256
LINE = 16
LIMIT = 24
STAGES = 4
DELAY = 3
AHEAD = 2
NORMS = 4
START = 0.12
UP_CUTS = 12
DOWN_CUTS = 6
SHARED = 19
SHARES = 32


def normalize(tokens):
    values = tokens.astype(jnp.float32)
    center = jnp.mean(values, axis=-1, keepdims=True)
    spread = jnp.mean(jnp.square(values - center), axis=-1, keepdims=True)
    return ((values - center) * lax.rsqrt(spread + 1e-05)).astype(jnp.bfloat16)


def pieces_of(size, unit, most):
    for count in range(most, 1, -1):
        if size % (count * unit) == 0:
            return count
    return 1


def shared_rows(height):
    return height * SHARED // SHARES // (2 * LINE) * (2 * LINE)


def order_of(fs, up_cuts, down_cuts, share):
    ready = []
    for cut in range(up_cuts):
        at = (cut + 1) / up_cuts
        ready.append((START + at, 0, "relay", 0, cut))
        for j, came in enumerate((START + at, START + 0.1 + 1.5 * at, START + 0.2 + 1.5 * at, START + 1.15 + at)):
            ready.append((came, 1, "arrive", j, cut))
    for cut in range(down_cuts):
        at = (cut + 1) / down_cuts
        ready.append((START + 1.05 + (1 - share) * at, 2, "split", 0, cut))
        ready.append((START + 1.05 + 1 - share + 2 * share * at, 4, "shared", 0, cut))
    ready.append((START + 0.3, 0, "send", 0, 0))
    ready.append((START + 0.6, 0, "send", 1, 0))
    ready.sort()
    order, spare, now = [], [], START
    for came, _, kind, j, cut in ready:
        while spare and kind == "arrive" and now + (1 - share) / down_cuts <= came:
            order.append(("cross", 0, spare.pop(0)))
            now += (1 - share) / down_cuts
        order.append((kind, j, cut))
        if kind == "arrive":
            now = max(now, came) + 2 / (fs * up_cuts)
        if kind == "split":
            spare.append(cut)
    last = max(i for i, entry in enumerate(order) if entry[0] == "arrive") + 1
    return order[:last], spare


def hand_over(dims, cuts, tokens_ref, gain_ref, up_ref, master_ref, got_up, got_down, out_ref, rows_ref, gains, up_stage, up_src, relayed, stage, hidden, hold, keep, send1, recv1, send2, recv2, up_sems, down_sems, sum_sems, load_sems):
    groups, fs, tp = dims
    up_cuts, down_cuts = cuts
    y, f, t = lax.axis_index("grp"), lax.axis_index("fs"), lax.axis_index("tp")
    x, k = t // CORES, t % CORES
    home_send, cross_send, relay_send, y_send, a_send, b_send, first_recv, relay_recv, y_recv, pair_recv = up_sems
    own_send, own_recv, split_send, shared_send, dy_send, da_send, ds_send, db_send, split_recv, shared_recv, dy_recv, twin_recv = down_sems
    send1_send, send1_recv, send2_send, send2_recv = sum_sems
    load_up, load_down, load_tokens = load_sems
    rows, cols = up_src.shape[1], up_src.shape[2] // up_cuts
    depth = got_up.shape[0] * got_up.shape[1] * got_up.shape[2]
    height, width = master_ref.shape
    tile = width // down_cuts
    both = shared_rows(height)
    part = (height - both) // groups
    near = f + 1 - 2 * (f % 2)
    rows_from = (f, near, (fs - 1) * (1 - f // 2), 2 - f // 2)
    facing = (f + 2) % fs
    sibling = (y, f, x * CORES + (1 - k))
    across_y = (1 - y, f, t)
    other = (1 - x) * CORES
    across_x = (y, f, other + k)

    def remote(src, dst, send, recv, where):
        return pltpu.make_async_remote_copy(src_ref=src, dst_ref=dst, send_sem=send, recv_sem=recv, device_id=where, device_id_type=MESH)

    def up_at(ref, group, lane, cut):
        return ref.at[group * CORES + lane, :, pl.ds(cut * cols, cols)]

    def src_at(lane, cut):
        return up_src.at[lane, :, pl.ds(cut * cols, cols)]

    def up_load(lane, cut):
        at = pl.ds(cut * cols, cols)
        return pltpu.make_async_copy(up_ref.at[y * CORES + lane, :, at], up_stage.at[lane, :, at], load_up.at[cut])

    def up_local(cut):
        return pltpu.make_async_copy(src_at(k, cut), up_at(got_up.at[f], y, k, cut), first_recv.at[f, cut])

    def up_home(lane, cut):
        return remote(src_at(lane, cut), up_at(got_up.at[f], y, lane, cut), home_send, first_recv.at[f, cut], (y, t, x * CORES + lane))

    def up_cross_own(lane, cut):
        return remote(src_at(lane, cut), up_at(got_up.at[f], y, lane, cut), cross_send, first_recv.at[f, cut], (y, f, other + lane))

    def up_cross(lane, cut):
        return remote(src_at(lane, cut), relayed.at[k, :, pl.ds(cut * cols, cols)], cross_send, relay_recv.at[k, cut], (y, f, other + lane))

    def up_relay(slot, cut):
        return remote(relayed.at[slot, :, pl.ds(cut * cols, cols)], up_at(got_up.at[f], y, k, cut), relay_send, first_recv.at[f, cut], (y, other + slot, t))

    def up_here(r, cut):
        return pltpu.make_async_copy(src_at(0, cut), up_at(got_up.at[r], y, k, cut), first_recv.at[r, cut])

    def relay_here(slot, cut):
        return pltpu.make_async_copy(src_at(0, cut), relayed.at[slot, :, pl.ds(cut * cols, cols)], relay_recv.at[slot, cut])

    def up_y(r, cut):
        here = up_at(got_up.at[r], y, k, cut)
        return remote(here, here, y_send, y_recv.at[r, cut], across_y)

    def up_a(r, cut):
        here = up_at(got_up.at[r], y, k, cut)
        return remote(here, here, a_send, pair_recv.at[cut], sibling)

    def up_b(r, cut):
        here = up_at(got_up.at[r], 1 - y, k, cut)
        return remote(here, here, b_send, pair_recv.at[cut], sibling)

    def tile_at(first, size, column, cut):
        return got_down.at[pl.ds(pl.multiple_of(first, LINE), size), pl.ds(pl.multiple_of(column * width + cut * tile, tile), tile)]

    def split_at(group, column, cut):
        return tile_at(group * part, part, column, cut)

    def shared_at(column, cut):
        return tile_at(groups * part, both, column, cut)

    def down_split(cut):
        here = split_at(y, t, cut)
        return remote(here, here, split_send, split_recv.at[cut], across_x)

    def down_shared(cut):
        here = shared_at(t, cut)
        return remote(here, here, shared_send, shared_recv.at[cut], across_x)

    def down_y(cut):
        here = split_at(y, other + k, cut)
        return remote(here, here, dy_send, dy_recv.at[cut], across_y)

    def down_a(cut):
        here = split_at(y, other + k, cut)
        return remote(here, here, da_send, twin_recv.at[cut], sibling)

    def down_s(cut):
        here = shared_at(other + k, cut)
        return remote(here, here, ds_send, twin_recv.at[cut], sibling)

    def down_b(cut):
        here = split_at(1 - y, other + k, cut)
        return remote(here, here, db_send, twin_recv.at[cut], sibling)

    own_columns = got_down.at[:, pl.ds(pl.multiple_of(t * width, width), width)]
    down_own = remote(own_columns, own_columns, own_send, own_recv, sibling)

    slab = stage.shape[1]
    slots = stage.shape[0]
    slabs = height // slab

    def take(step):
        return pltpu.make_async_copy(master_ref.at[pl.ds(step * slab, slab), :], stage.at[step % slots], load_down.at[step % slots])

    take_tokens = pltpu.make_async_copy(tokens_ref, rows_ref, load_tokens)

    for cut in range(up_cuts):
        for lane in range(CORES):
            up_load(lane, cut).start()
    for step in range(slots):
        take(step).start()
    take_tokens.start()

    barrier = pltpu.get_barrier_semaphore()
    partners = [sibling, across_y] + [(y, f, other + lane) for lane in range(CORES)]
    partners += [(y, rows_from[j], x * CORES + lane) for j in range(1, fs) for lane in range(CORES)]
    for partner in partners:
        pl.semaphore_signal(barrier, inc=1, device_id=partner, device_id_type=MESH)

    gains[...] = jnp.transpose(jnp.broadcast_to(gain_ref[...][None, :], (128, gain_ref.shape[0])))

    def up_cast(cut):
        whole = up_stage.at[:, :, pl.ds(cut * cols, cols)]
        pltpu.make_async_copy(whole, whole, load_up.at[cut]).wait()
        for lane in range(CORES):
            @pl.loop(0, rows // LINE)
            def _(line):
                at = pl.ds(pl.multiple_of(line * LINE, LINE), LINE)
                scale = gains[pl.ds(pl.multiple_of((y * CORES + lane) * rows + line * LINE, LINE), LINE), :]
                block = up_stage[lane, at, pl.ds(cut * cols, cols)]
                up_src[lane, at, pl.ds(cut * cols, cols)] = (jnp.concatenate([scale] * (cols // 128), axis=1) * block).astype(jnp.bfloat16)

    def up_start(cut):
        for lane in range(CORES):
            @pl.when(t == f)
            def _():
                up_cross_own(lane, cut).start()

            @pl.when(t != f)
            def _():
                up_cross(lane, cut).start()

    def up_direct(cut):
        for lane in range(CORES):
            @pl.when(jnp.logical_or(t != f, lane != k))
            def _():
                up_home(lane, cut).start()

        @pl.when(t == f)
        def _():
            up_local(cut).start()

    for cut in range(up_cuts):
        up_cast(cut)
    pl.semaphore_wait(barrier, len(partners))
    for cut in range(up_cuts):
        up_start(cut)
        if cut == 0:
            up_direct(cut)

    def down_cast(step):
        take(step).wait()

        @pl.loop(0, slab // LINE)
        def _(line):
            start = pl.multiple_of(line * LINE, LINE)
            to = pl.ds(pl.multiple_of(step * slab + start, LINE), LINE)
            got_down[to, pl.ds(pl.multiple_of(t * width, width), width)] = stage[step % slots, pl.ds(start, LINE), :].astype(jnp.bfloat16)

        if step + slots < slabs:
            take(step + slots).start()
        if step == slabs - 1:
            down_own.start()

    def normalize_rows(step):
        if step == 0:
            take_tokens.wait()
        span = tokens_ref.shape[0] // NORMS

        @pl.loop(0, span // LINE)
        def _(line):
            at = pl.ds(pl.multiple_of(step * span + line * LINE, LINE), LINE)
            rows_ref[at, :] = normalize(rows_ref[at, :])

    def hidden_units(cut):
        @pl.loop(0, cols // UNIT)
        def _(step):
            at = pl.ds(pl.multiple_of(cut * cols + step * UNIT, UNIT), UNIT)
            block = got_up[:, :, :, at].reshape(depth, UNIT)
            before = jnp.dot(rows_ref[...], block, preferred_element_type=jnp.float32)
            hidden[:, at] = jnp.square(jnp.maximum(before, 0.0)).astype(jnp.bfloat16)

    def up_arrive(j, cut):
        r = rows_from[j]
        up_here(r, cut).wait()
        up_y(r, cut).start()
        up_a(r, cut).start()

    def up_second(j, cut):
        r = rows_from[j]
        up_y(r, cut).wait_recv()
        up_b(r, cut).start()

    def up_done(cut):
        landed = got_up.at[:, pl.ds(0, groups), :, pl.ds(cut * cols, cols)]
        pltpu.make_async_copy(landed, landed, pair_recv.at[cut]).wait()
        hidden_units(cut)

    def sum_near(g, cut):
        at = pl.ds(cut * tile, tile)
        return remote(send1.at[g, :, at], recv1.at[g, :, at], send1_send, send1_recv.at[g, cut], (y, near, t))

    def sum_far(cut):
        at = pl.ds(cut * tile, tile)
        return remote(send2.at[:, at], recv2.at[:, at], send2_send, send2_recv.at[cut], (y, facing, t))

    bases = (x * CORES, other)
    close = x == f // CORES
    kept = (x + f // CORES) % PLANES

    def terms(g, cut, first, last):
        away, here = (pl.ds(pl.multiple_of(column * width + cut * tile, tile), tile) for column in (bases[g] + 1 - f % 2, bases[g] + f % 2))
        total = jnp.zeros((hidden.shape[0], 2 * tile), jnp.float32)
        for unit in range(first, last, UNIT):
            at = pl.ds(unit, UNIT)
            block = jnp.concatenate([got_down[at, away], got_down[at, here]], axis=1)
            total += jnp.dot(hidden[:, at], block, preferred_element_type=jnp.float32)
        return total[:, :tile], total[:, tile:]

    def features(g, cut, first, last):
        at = pl.ds(cut * tile, tile)
        away, here = terms(g, cut, first, last)
        if first > 0:
            away, here = hold[:, at] + away, keep[g, :, at] + here
        keep[g, :, at] = here
        if last == height:
            send1[g, :, at] = away.astype(jnp.bfloat16)
            if g == 1 or cut < AHEAD:
                sum_near(g, cut).start()
            else:
                @pl.when(jnp.logical_not(close))
                def _():
                    sum_near(g, cut).start()
        else:
            hold[:, at] = away

    def pass_on(g, cut):
        at = pl.ds(cut * tile, tile)
        sum_near(g, cut).wait_recv()
        send2[:, at] = (keep[g, :, at] + recv1[g, :, at].astype(jnp.float32)).astype(jnp.bfloat16)
        sum_far(cut).start()

    def finish(cut):
        at = pl.ds(cut * tile, tile)
        sum_near(kept, cut).wait_recv()
        sum_far(cut).wait_recv()
        total = keep[kept, :, at] + recv1[kept, :, at].astype(jnp.float32) + recv2[:, at].astype(jnp.float32)
        out_ref[:, at] = total.astype(jnp.bfloat16)

    def twin_in(cut):
        landed = tile_at(0, height, other + (1 - k), cut)
        pltpu.make_async_copy(landed, landed, twin_recv.at[cut]).wait()

    def sent(ref, sem):
        pltpu.make_async_copy(ref, ref, sem).wait()

    def drain():
        sent(up_src, cross_send)

        @pl.when(t == f)
        def _():
            sent(up_src.at[0], home_send)

        @pl.when(t != f)
        def _():
            sent(up_src, home_send)

        @pl.when(jnp.logical_or(other == f, other + 1 == f))
        def _():
            sent(relayed.at[0], relay_send)

        @pl.when(jnp.logical_and(other != f, other + 1 != f))
        def _():
            sent(relayed, relay_send)

        for sem in (y_send, a_send, b_send):
            sent(got_up.at[:, 0], sem)
        sent(own_columns, own_send)
        for sem in (split_send, dy_send, da_send, db_send):
            sent(got_down.at[pl.ds(0, part), pl.ds(0, width)], sem)
        for sem in (shared_send, ds_send):
            sent(got_down.at[pl.ds(0, both), pl.ds(0, width)], sem)

    waiting, seen, ready, crossed, shared = [], [0] * up_cuts, [], [], []
    tasks = [functools.partial(down_cast, step) for step in range(slabs)] + [functools.partial(normalize_rows, step) for step in range(NORMS)]
    stages = STAGES if up_cuts % STAGES == 0 and height == up_cuts * cols else 1
    span = up_cuts // stages

    def finished(cut):
        up_done(cut)
        if (cut + 1) % span == 0 and cut + 1 < up_cuts:
            if cut + 1 == span:
                tasks.append(down_own.wait_recv)
            for piece in range(down_cuts):
                tasks.append(functools.partial(features, 0, piece, (cut + 1 - span) * cols, (cut + 1) * cols))

    def spend(count):
        for _ in range(min(count, len(tasks))):
            tasks.pop(0)()

    def follow():
        kind, j, cut = waiting.pop(0)
        if kind == "cross":
            down_y(cut).wait_recv()
            down_b(cut).start()
            crossed.append(cut)
        else:
            up_second(j, cut)
            seen[cut] += 1
            if seen[cut] == fs:
                ready.append(cut)

    def shared_in(cut):
        down_shared(cut).wait_recv()
        down_s(cut).start()
        shared.append(cut)

    order, late = order_of(fs, up_cuts, down_cuts, both / height)
    for kind, j, cut in order:
        if kind == "relay":
            for slot in range(CORES):
                @pl.when(other + slot != f)
                def _():
                    relay_here(slot, cut).wait()
                    up_relay(slot, cut).start()

            if cut + 1 < up_cuts:
                up_direct(cut + 1)
            spend(1)
        elif kind == "send":
            if j == 0:
                spend(len(tasks))
            for piece in range(down_cuts):
                (down_split, down_shared)[j](piece).start()
        elif kind == "split":
            down_split(cut).wait_recv()
            down_a(cut).start()
        elif kind == "shared":
            shared_in(cut)
        else:
            if kind == "cross":
                down_y(cut).start()
            else:
                up_arrive(j, cut)
            waiting.append((kind, j, cut))
            if len(waiting) > LAG:
                follow()
            if len(ready) > 1:
                finished(ready.pop(0))
            else:
                spend(1)

    for cut in late:
        down_y(cut).start()
        waiting.append(("cross", 0, cut))
    while sum(seen) < fs * up_cuts:
        follow()
        spend(2)
        while ready:
            finished(ready.pop(0))
    spend(len(tasks))
    if stages == 1:
        down_own.wait_recv()
    for cut in range(down_cuts):
        features(0, cut, height - height // stages, height)

    def cross_in(step):
        while step not in crossed:
            follow()

    for step in range(down_cuts):
        if step not in shared:
            shared_in(step)
        cross_in(step)
        @pl.when(jnp.logical_not(close))
        def _():
            pass_on(0, step)

        if step >= DELAY:
            @pl.when(close)
            def _():
                pass_on(1, step - DELAY)

        twin_in(step)
        features(1, step, 0, height)
        if step + AHEAD < down_cuts:
            @pl.when(close)
            def _():
                sum_near(0, step + AHEAD).start()

    @pl.when(close)
    def _():
        for step in range(down_cuts - DELAY, down_cuts):
            pass_on(1, step)

    drain()
    for step in range(1, down_cuts):
        finish(step - 1)
    finish(down_cuts - 1)
    sent(send1, send1_send)
    sent(send2, send2_send)


def put_out(src_ref, out_ref, sems):
    chunks = sems.shape[0]
    step = src_ref.shape[0] // chunks
    for chunk in range(chunks):
        at = pl.ds(chunk * step, step)
        pltpu.make_async_copy(src_ref.at[at], out_ref.at[at], sems.at[chunk]).start()
    for chunk in range(chunks):
        at = pl.ds(chunk * step, step)
        pltpu.make_async_copy(src_ref.at[at], out_ref.at[at], sems.at[chunk]).wait()


def put(array):
    return pl.pallas_call(
        put_out,
        out_shape=jax.ShapeDtypeStruct(array.shape, array.dtype),
        in_specs=[pl.BlockSpec(memory_space=pltpu.VMEM)],
        out_specs=pl.BlockSpec(memory_space=pltpu.HBM),
        scratch_shapes=[pltpu.SemaphoreType.DMA((4,))],
        compiler_params=pltpu.CompilerParams(vmem_limit_bytes=1 << 20),
    )(array)


def fused(tokens_in, up_master, down_master, norm_gain, dims):
    groups, fs, tp = dims
    rows, cols = up_master.shape[0] // (groups * CORES), up_master.shape[1]
    height, width = down_master.shape
    tokens = tokens_in.shape[0]
    up_cuts = pieces_of(cols, UNIT, UP_CUTS)
    down_cuts = pieces_of(width, 128, DOWN_CUTS)
    slabs = pieces_of(height, LINE, 8)
    dma = pltpu.SemaphoreType.DMA
    lanes, whole, strip = dma((CORES, up_cuts)), dma((fs, up_cuts)), dma((down_cuts,))
    up_sems = [dma] * 6 + [whole, lanes, whole, dma((up_cuts,))]
    down_sems = [dma] * 8 + [strip] * 4
    sum_sems = [dma, dma((2, down_cuts)), dma, strip]
    vmem = pl.BlockSpec(memory_space=pltpu.VMEM)
    hbm = pl.BlockSpec(memory_space=pl.ANY)
    got_up, got_down, out = pl.pallas_call(
        functools.partial(hand_over, dims, (up_cuts, down_cuts)),
        out_shape=(
            pltpu.VMEM((fs, groups * CORES, rows, cols), jnp.bfloat16),
            pltpu.VMEM((height, tp * width), jnp.bfloat16),
            jax.ShapeDtypeStruct((tokens, width), jnp.bfloat16),
        ),
        in_specs=[hbm, vmem, hbm, hbm],
        out_specs=(vmem, vmem, vmem),
        scratch_shapes=[
            pltpu.VMEM(tokens_in.shape, jnp.bfloat16),
            pltpu.VMEM((up_master.shape[0], 128), jnp.float32),
            pltpu.VMEM((CORES, rows, cols), jnp.float32),
            pltpu.VMEM((CORES, rows, cols), jnp.bfloat16),
            pltpu.VMEM((CORES, rows, cols), jnp.bfloat16),
            pltpu.VMEM((2, height // slabs, width), jnp.float32),
            pltpu.VMEM((tokens, cols), jnp.bfloat16),
            pltpu.VMEM((tokens, width), jnp.float32),
            pltpu.VMEM((2, tokens, width), jnp.float32),
            pltpu.VMEM((2, tokens, width), jnp.bfloat16),
            pltpu.VMEM((2, tokens, width), jnp.bfloat16),
            pltpu.VMEM((tokens, width), jnp.bfloat16),
            pltpu.VMEM((tokens, width), jnp.bfloat16),
            up_sems,
            down_sems,
            sum_sems,
            [dma((up_cuts,)), dma((2,)), dma],
        ],
        compiler_params=pltpu.CompilerParams(collective_id=0, has_side_effects=True, vmem_limit_bytes=LIMIT << 20),
    )(tokens_in, norm_gain, up_master.reshape(groups * CORES, rows, cols), down_master)
    return out, put(got_up).reshape(fs * groups * CORES * rows, cols), put(got_down)


def fits(up_shape, down_shape, dims):
    groups, fs, tp = dims
    own = 2 * (up_shape[0] * up_shape[1] * fs + down_shape[0] * down_shape[1] * tp)
    aligned = up_shape[0] % (groups * CORES * LINE) == 0 and up_shape[0] % 128 == 0 and up_shape[1] % UNIT == 0
    square = groups == 2 and tp == CORES * PLANES and fs == tp
    return square and aligned and down_shape[0] % UNIT == 0 and down_shape[1] % 128 == 0 and own <= 40 << 20


def by_collectives(normalized, up_cast, down_cast):
    quarter = lax.all_to_all(up_cast, "tp", split_axis=0, concat_axis=1, tiled=True)
    moved = lax.all_to_all(quarter, "fs", split_axis=1, concat_axis=0, tiled=True)
    part_rows = quarter.shape[0]
    stacked = moved.reshape(moved.shape[0] // part_rows, part_rows, moved.shape[1])
    joined = lax.all_gather(stacked, "tp", axis=1, tiled=True)
    sampled_down = lax.all_gather(down_cast, "tp", axis=1, tiled=True)
    sampled_up = joined.reshape(joined.shape[0] * joined.shape[1], joined.shape[2])
    before = jnp.dot(normalized, sampled_up, preferred_element_type=jnp.float32)
    hidden = jnp.square(jax.nn.relu(before)).astype(jnp.bfloat16)
    terms = jnp.dot(hidden, sampled_down, preferred_element_type=jnp.float32)
    summed = lax.psum_scatter(terms, "fs", scatter_dimension=1, tiled=True)
    return summed.astype(jnp.bfloat16), sampled_up, sampled_down


def shards(dims, tokens, up_master, down_master, norm_gain):
    if fits(up_master.shape, down_master.shape, dims):
        return fused(tokens, up_master, down_master, norm_gain, dims)
    up_cast = (norm_gain[:, None] * up_master).astype(jnp.bfloat16)
    return by_collectives(normalize(tokens), up_cast, down_master.astype(jnp.bfloat16))


def solution(mesh):
    dims = tuple(mesh.shape[name] for name in ("grp", "fs", "tp"))
    return jax.shard_map(
        functools.partial(shards, dims),
        mesh=mesh,
        in_specs=(P(("grp", "tp"), None), P("fs", "tp"), P("fs", "tp"), P("fs")),
        out_specs=(P(("grp", "tp"), "fs"), P("grp", "fs"), P(("grp", "fs"), None)),
        check_vma=False,
    )
```

```python
import functools

import jax
import jax.numpy as jnp
from jax import lax
from jax.experimental import pallas as pl
from jax.experimental.pallas import tpu as pltpu
from jax.sharding import PartitionSpec as P

MESH = pl.DeviceIdType.MESH
CORES = 2
PLANES = 2
LAG = 3
UNIT = 256
LINE = 16
LIMIT = 24
STAGES = 4
DELAY = 3
AHEAD = 2
LATE = 2
FLOPS = 10_000_000_000
NORMS = 4
START = 0.12
UP_CUTS = 12
DOWN_CUTS = 6
SHARED = 19
SHARES = 32


def normalize(tokens):
    values = tokens.astype(jnp.float32)
    center = jnp.mean(values, axis=-1, keepdims=True)
    spread = jnp.mean(jnp.square(values - center), axis=-1, keepdims=True)
    return ((values - center) * lax.rsqrt(spread + 1e-05)).astype(jnp.bfloat16)


def pieces_of(size, unit, most):
    for count in range(most, 1, -1):
        if size % (count * unit) == 0:
            return count
    return 1


def shared_rows(height):
    return height * SHARED // SHARES // (2 * LINE) * (2 * LINE)


def order_of(fs, up_cuts, down_cuts, share):
    ready = []
    for cut in range(up_cuts):
        at = (cut + 1) / up_cuts
        ready.append((START + at, 0, "relay", 0, cut))
        for j, came in enumerate((START + at, START + 0.1 + 1.5 * at, START + 0.2 + 1.5 * at, START + 1.15 + at)):
            ready.append((came, 1, "arrive", j, cut))
    for cut in range(down_cuts):
        at = (cut + 1) / down_cuts
        ready.append((START + 1.05 + (1 - share) * at, 2, "split", 0, cut))
        ready.append((START + 1.05 + 1 - share + 2 * share * at, 4, "shared", 0, cut))
    ready.append((START + 0.3, 0, "send", 0, 0))
    ready.append((START + 0.6, 0, "send", 1, 0))
    ready.sort()
    order, spare, now = [], [], START
    for came, _, kind, j, cut in ready:
        while spare and kind == "arrive" and now + (1 - share) / down_cuts <= came:
            order.append(("cross", 0, spare.pop(0)))
            now += (1 - share) / down_cuts
        order.append((kind, j, cut))
        if kind == "arrive":
            now = max(now, came) + 2 / (fs * up_cuts)
        if kind == "split":
            spare.append(cut)
    last = max(i for i, entry in enumerate(order) if entry[0] == "arrive") + 1
    return order[:last], spare


def hand_over(dims, cuts, tokens_ref, gain_ref, up_ref, master_ref, got_up, got_down, out_ref, base_ref, late_ref, away_ref, rows_ref, gains, up_stage, up_src, relayed, stage, hidden, hold, keep, send1, recv1, send2, recv2, up_sems, down_sems, sum_sems, load_sems):
    groups, fs, tp = dims
    up_cuts, down_cuts = cuts
    y, f, t = lax.axis_index("grp"), lax.axis_index("fs"), lax.axis_index("tp")
    x, k = t // CORES, t % CORES
    home_send, cross_send, relay_send, y_send, a_send, b_send, first_recv, relay_recv, y_recv, pair_recv = up_sems
    own_send, own_recv, split_send, shared_send, dy_send, da_send, ds_send, db_send, split_recv, shared_recv, dy_recv, twin_recv = down_sems
    send1_send, send1_recv, send2_send, send2_recv = sum_sems
    load_up, load_down, load_tokens = load_sems
    rows, cols = up_src.shape[1], up_src.shape[2] // up_cuts
    depth = got_up.shape[0] * got_up.shape[1] * got_up.shape[2]
    height, width = master_ref.shape
    tile = width // down_cuts
    both = shared_rows(height)
    part = (height - both) // groups
    near = f + 1 - 2 * (f % 2)
    rows_from = (f, near, (fs - 1) * (1 - f // 2), 2 - f // 2)
    facing = (f + 2) % fs
    sibling = (y, f, x * CORES + (1 - k))
    across_y = (1 - y, f, t)
    other = (1 - x) * CORES
    across_x = (y, f, other + k)

    def remote(src, dst, send, recv, where):
        return pltpu.make_async_remote_copy(src_ref=src, dst_ref=dst, send_sem=send, recv_sem=recv, device_id=where, device_id_type=MESH)

    def up_at(ref, group, lane, cut):
        return ref.at[group * CORES + lane, :, pl.ds(cut * cols, cols)]

    def src_at(lane, cut):
        return up_src.at[lane, :, pl.ds(cut * cols, cols)]

    def up_load(lane, cut):
        at = pl.ds(cut * cols, cols)
        return pltpu.make_async_copy(up_ref.at[y * CORES + lane, :, at], up_stage.at[lane, :, at], load_up.at[cut])

    def up_local(cut):
        return pltpu.make_async_copy(src_at(k, cut), up_at(got_up.at[f], y, k, cut), first_recv.at[f, cut])

    def up_home(lane, cut):
        return remote(src_at(lane, cut), up_at(got_up.at[f], y, lane, cut), home_send, first_recv.at[f, cut], (y, t, x * CORES + lane))

    def up_cross_own(lane, cut):
        return remote(src_at(lane, cut), up_at(got_up.at[f], y, lane, cut), cross_send, first_recv.at[f, cut], (y, f, other + lane))

    def up_cross(lane, cut):
        return remote(src_at(lane, cut), relayed.at[k, :, pl.ds(cut * cols, cols)], cross_send, relay_recv.at[k, cut], (y, f, other + lane))

    def up_relay(slot, cut):
        return remote(relayed.at[slot, :, pl.ds(cut * cols, cols)], up_at(got_up.at[f], y, k, cut), relay_send, first_recv.at[f, cut], (y, other + slot, t))

    def up_here(r, cut):
        return pltpu.make_async_copy(src_at(0, cut), up_at(got_up.at[r], y, k, cut), first_recv.at[r, cut])

    def relay_here(slot, cut):
        return pltpu.make_async_copy(src_at(0, cut), relayed.at[slot, :, pl.ds(cut * cols, cols)], relay_recv.at[slot, cut])

    def up_y(r, cut):
        here = up_at(got_up.at[r], y, k, cut)
        return remote(here, here, y_send, y_recv.at[r, cut], across_y)

    def up_a(r, cut):
        here = up_at(got_up.at[r], y, k, cut)
        return remote(here, here, a_send, pair_recv.at[cut], sibling)

    def up_b(r, cut):
        here = up_at(got_up.at[r], 1 - y, k, cut)
        return remote(here, here, b_send, pair_recv.at[cut], sibling)

    def tile_at(first, size, column, cut):
        return got_down.at[pl.ds(pl.multiple_of(first, LINE), size), pl.ds(pl.multiple_of(column * width + cut * tile, tile), tile)]

    def split_at(group, column, cut):
        return tile_at(group * part, part, column, cut)

    def shared_at(column, cut):
        return tile_at(groups * part, both, column, cut)

    def down_split(cut):
        here = split_at(y, t, cut)
        return remote(here, here, split_send, split_recv.at[cut], across_x)

    def down_shared(cut):
        here = shared_at(t, cut)
        return remote(here, here, shared_send, shared_recv.at[cut], across_x)

    def down_y(cut):
        here = split_at(y, other + k, cut)
        return remote(here, here, dy_send, dy_recv.at[cut], across_y)

    def down_a(cut):
        here = split_at(y, other + k, cut)
        return remote(here, here, da_send, twin_recv.at[cut], sibling)

    def down_s(cut):
        here = shared_at(other + k, cut)
        return remote(here, here, ds_send, twin_recv.at[cut], sibling)

    def down_b(cut):
        here = split_at(1 - y, other + k, cut)
        return remote(here, here, db_send, twin_recv.at[cut], sibling)

    own_columns = got_down.at[:, pl.ds(pl.multiple_of(t * width, width), width)]
    down_own = remote(own_columns, own_columns, own_send, own_recv, sibling)

    slab = stage.shape[1]
    slots = stage.shape[0]
    slabs = height // slab

    def take(step):
        return pltpu.make_async_copy(master_ref.at[pl.ds(step * slab, slab), :], stage.at[step % slots], load_down.at[step % slots])

    take_tokens = pltpu.make_async_copy(tokens_ref, rows_ref, load_tokens)

    for cut in range(up_cuts):
        for lane in range(CORES):
            up_load(lane, cut).start()
    for step in range(slots):
        take(step).start()
    take_tokens.start()

    barrier = pltpu.get_barrier_semaphore()
    partners = [sibling, across_y] + [(y, f, other + lane) for lane in range(CORES)]
    partners += [(y, rows_from[j], x * CORES + lane) for j in range(1, fs) for lane in range(CORES)]
    for partner in partners:
        pl.semaphore_signal(barrier, inc=1, device_id=partner, device_id_type=MESH)

    gains[...] = jnp.transpose(jnp.broadcast_to(gain_ref[...][None, :], (128, gain_ref.shape[0])))

    def up_cast(cut):
        whole = up_stage.at[:, :, pl.ds(cut * cols, cols)]
        pltpu.make_async_copy(whole, whole, load_up.at[cut]).wait()
        for lane in range(CORES):
            @pl.loop(0, rows // LINE)
            def _(line):
                at = pl.ds(pl.multiple_of(line * LINE, LINE), LINE)
                scale = gains[pl.ds(pl.multiple_of((y * CORES + lane) * rows + line * LINE, LINE), LINE), :]
                block = up_stage[lane, at, pl.ds(cut * cols, cols)]
                up_src[lane, at, pl.ds(cut * cols, cols)] = (jnp.concatenate([scale] * (cols // 128), axis=1) * block).astype(jnp.bfloat16)

    def up_start(cut):
        for lane in range(CORES):
            @pl.when(t == f)
            def _():
                up_cross_own(lane, cut).start()

            @pl.when(t != f)
            def _():
                up_cross(lane, cut).start()

    def up_direct(cut):
        for lane in range(CORES):
            @pl.when(jnp.logical_or(t != f, lane != k))
            def _():
                up_home(lane, cut).start()

        @pl.when(t == f)
        def _():
            up_local(cut).start()

    for cut in range(up_cuts):
        up_cast(cut)
    pl.semaphore_wait(barrier, len(partners))
    for cut in range(up_cuts):
        up_start(cut)
        if cut == 0:
            up_direct(cut)

    def down_cast(step):
        take(step).wait()

        @pl.loop(0, slab // LINE)
        def _(line):
            start = pl.multiple_of(line * LINE, LINE)
            to = pl.ds(pl.multiple_of(step * slab + start, LINE), LINE)
            got_down[to, pl.ds(pl.multiple_of(t * width, width), width)] = stage[step % slots, pl.ds(start, LINE), :].astype(jnp.bfloat16)

        if step + slots < slabs:
            take(step + slots).start()
        if step == slabs - 1:
            down_own.start()

    def normalize_rows(step):
        if step == 0:
            take_tokens.wait()
        span = tokens_ref.shape[0] // NORMS

        @pl.loop(0, span // LINE)
        def _(line):
            at = pl.ds(pl.multiple_of(step * span + line * LINE, LINE), LINE)
            rows_ref[at, :] = normalize(rows_ref[at, :])

    def hidden_units(cut):
        @pl.loop(0, cols // UNIT)
        def _(step):
            at = pl.ds(pl.multiple_of(cut * cols + step * UNIT, UNIT), UNIT)
            block = got_up[:, :, :, at].reshape(depth, UNIT)
            before = jnp.dot(rows_ref[...], block, preferred_element_type=jnp.float32)
            hidden[:, at] = jnp.square(jnp.maximum(before, 0.0)).astype(jnp.bfloat16)

    def up_arrive(j, cut):
        r = rows_from[j]
        up_here(r, cut).wait()
        up_y(r, cut).start()
        up_a(r, cut).start()

    def up_second(j, cut):
        r = rows_from[j]
        up_y(r, cut).wait_recv()
        up_b(r, cut).start()

    def up_done(cut):
        landed = got_up.at[:, pl.ds(0, groups), :, pl.ds(cut * cols, cols)]
        pltpu.make_async_copy(landed, landed, pair_recv.at[cut]).wait()
        hidden_units(cut)

    def sum_near(g, cut):
        at = pl.ds(cut * tile, tile)
        return remote(send1.at[g, :, at], recv1.at[g, :, at], send1_send, send1_recv.at[g, cut], (y, near, t))

    def sum_far(cut):
        at = pl.ds(cut * tile, tile)
        return remote(send2.at[:, at], recv2.at[:, at], send2_send, send2_recv.at[cut], (y, facing, t))

    bases = (x * CORES, other)
    soon = down_cuts - LATE
    close = x == f // CORES
    kept = (x + f // CORES) % PLANES

    def terms(g, cut, first, last):
        away, here = (pl.ds(pl.multiple_of(column * width + cut * tile, tile), tile) for column in (bases[g] + 1 - f % 2, bases[g] + f % 2))
        total = jnp.zeros((hidden.shape[0], 2 * tile), jnp.float32)
        for unit in range(first, last, UNIT):
            at = pl.ds(unit, UNIT)
            block = jnp.concatenate([got_down[at, away], got_down[at, here]], axis=1)
            total += jnp.dot(hidden[:, at], block, preferred_element_type=jnp.float32)
        return total[:, :tile], total[:, tile:]

    def features(g, cut, first, last):
        at = pl.ds(cut * tile, tile)
        away, here = terms(g, cut, first, last)
        if g == 1 and cut >= soon:
            place = pl.ds((cut - soon) * tile, tile)
            late_ref[:, place] = here
            away_ref[:, place] = away.astype(jnp.bfloat16)
            return
        if first > 0:
            away, here = hold[:, at] + away, keep[g, :, at] + here
        keep[g, :, at] = here
        if last == height:
            send1[g, :, at] = away.astype(jnp.bfloat16)
            if g == 1 or cut < AHEAD:
                sum_near(g, cut).start()
            else:
                @pl.when(jnp.logical_not(close))
                def _():
                    sum_near(g, cut).start()
        else:
            hold[:, at] = away

    def pass_on(g, cut):
        at = pl.ds(cut * tile, tile)
        sum_near(g, cut).wait_recv()
        send2[:, at] = (keep[g, :, at] + recv1[g, :, at].astype(jnp.float32)).astype(jnp.bfloat16)
        sum_far(cut).start()

    def finish(cut):
        at = pl.ds(cut * tile, tile)
        sum_near(kept, cut).wait_recv()
        sum_far(cut).wait_recv()
        total = keep[kept, :, at] + recv1[kept, :, at].astype(jnp.float32) + recv2[:, at].astype(jnp.float32)
        if cut < soon:
            out_ref[:, at] = total.astype(jnp.bfloat16)
        else:
            base_ref[:, pl.ds((cut - soon) * tile, tile)] = total

    def twin_in(cut):
        landed = tile_at(0, height, other + (1 - k), cut)
        pltpu.make_async_copy(landed, landed, twin_recv.at[cut]).wait()

    def sent(ref, sem):
        pltpu.make_async_copy(ref, ref, sem).wait()

    def drain():
        sent(up_src, cross_send)

        @pl.when(t == f)
        def _():
            sent(up_src.at[0], home_send)

        @pl.when(t != f)
        def _():
            sent(up_src, home_send)

        @pl.when(jnp.logical_or(other == f, other + 1 == f))
        def _():
            sent(relayed.at[0], relay_send)

        @pl.when(jnp.logical_and(other != f, other + 1 != f))
        def _():
            sent(relayed, relay_send)

        for sem in (y_send, a_send, b_send):
            sent(got_up.at[:, 0], sem)
        sent(own_columns, own_send)
        for sem in (split_send, dy_send, da_send, db_send):
            sent(got_down.at[pl.ds(0, part), pl.ds(0, width)], sem)
        for sem in (shared_send, ds_send):
            sent(got_down.at[pl.ds(0, both), pl.ds(0, width)], sem)

    waiting, seen, ready, crossed, shared = [], [0] * up_cuts, [], [], []
    tasks = [functools.partial(down_cast, step) for step in range(slabs)] + [functools.partial(normalize_rows, step) for step in range(NORMS)]
    stages = STAGES if up_cuts % STAGES == 0 and height == up_cuts * cols else 1
    span = up_cuts // stages

    def finished(cut):
        up_done(cut)
        if (cut + 1) % span == 0 and cut + 1 < up_cuts:
            if cut + 1 == span:
                tasks.append(down_own.wait_recv)
            for piece in range(down_cuts):
                tasks.append(functools.partial(features, 0, piece, (cut + 1 - span) * cols, (cut + 1) * cols))

    def spend(count):
        for _ in range(min(count, len(tasks))):
            tasks.pop(0)()

    def follow():
        kind, j, cut = waiting.pop(0)
        if kind == "cross":
            down_y(cut).wait_recv()
            down_b(cut).start()
            crossed.append(cut)
        else:
            up_second(j, cut)
            seen[cut] += 1
            if seen[cut] == fs:
                ready.append(cut)

    def shared_in(cut):
        down_shared(cut).wait_recv()
        down_s(cut).start()
        shared.append(cut)

    order, late = order_of(fs, up_cuts, down_cuts, both / height)
    for kind, j, cut in order:
        if kind == "relay":
            for slot in range(CORES):
                @pl.when(other + slot != f)
                def _():
                    relay_here(slot, cut).wait()
                    up_relay(slot, cut).start()

            if cut + 1 < up_cuts:
                up_direct(cut + 1)
            spend(1)
        elif kind == "send":
            if j == 0:
                spend(len(tasks))
            for piece in range(down_cuts):
                (down_split, down_shared)[j](piece).start()
        elif kind == "split":
            down_split(cut).wait_recv()
            down_a(cut).start()
        elif kind == "shared":
            shared_in(cut)
        else:
            if kind == "cross":
                down_y(cut).start()
            else:
                up_arrive(j, cut)
            waiting.append((kind, j, cut))
            if len(waiting) > LAG:
                follow()
            if len(ready) > 1:
                finished(ready.pop(0))
            else:
                spend(1)

    for cut in late:
        down_y(cut).start()
        waiting.append(("cross", 0, cut))
    while sum(seen) < fs * up_cuts:
        follow()
        spend(2)
        while ready:
            finished(ready.pop(0))
    spend(len(tasks))
    if stages == 1:
        down_own.wait_recv()
    for cut in range(down_cuts):
        features(0, cut, height - height // stages, height)

    def cross_in(step):
        while step not in crossed:
            follow()

    for step in range(down_cuts):
        if step not in shared:
            shared_in(step)
        cross_in(step)
        @pl.when(jnp.logical_not(close))
        def _():
            pass_on(0, step)

        if DELAY <= step < DELAY + soon:
            @pl.when(close)
            def _():
                pass_on(1, step - DELAY)

        twin_in(step)
        features(1, step, 0, height)
        if step + AHEAD < down_cuts:
            @pl.when(close)
            def _():
                sum_near(0, step + AHEAD).start()

    @pl.when(close)
    def _():
        for step in range(max(down_cuts - DELAY, 0), soon):
            pass_on(1, step)

    drain()
    for step in range(soon):
        finish(step)

    sent(rows_ref.at[:, pl.ds(0, (down_cuts + soon) * tile)], send1_send)

    @pl.when(close)
    def _():
        for step in range(soon, down_cuts):
            finish(step)
        if soon:
            sent(send2.at[:, pl.ds(0, soon * tile)], send2_send)

    @pl.when(jnp.logical_not(close))
    def _():
        base_ref[...] = jnp.zeros_like(base_ref)
        sent(send2, send2_send)


def put_out(src_ref, out_ref, sems):
    chunks = sems.shape[0]
    step = src_ref.shape[0] // chunks
    for chunk in range(chunks):
        at = pl.ds(chunk * step, step)
        pltpu.make_async_copy(src_ref.at[at], out_ref.at[at], sems.at[chunk]).start()
    for chunk in range(chunks):
        at = pl.ds(chunk * step, step)
        pltpu.make_async_copy(src_ref.at[at], out_ref.at[at], sems.at[chunk]).wait()


def put(array):
    return pl.pallas_call(
        put_out,
        out_shape=jax.ShapeDtypeStruct(array.shape, array.dtype),
        in_specs=[pl.BlockSpec(memory_space=pltpu.VMEM)],
        out_specs=pl.BlockSpec(memory_space=pltpu.HBM),
        scratch_shapes=[pltpu.SemaphoreType.DMA((4,))],
        compiler_params=pltpu.CompilerParams(vmem_limit_bytes=1 << 20),
        cost_estimate=pl.CostEstimate(flops=FLOPS, bytes_accessed=2 * array.size, transcendentals=0),
    )(array)


def fused(tokens_in, up_master, down_master, norm_gain, dims):
    groups, fs, tp = dims
    rows, cols = up_master.shape[0] // (groups * CORES), up_master.shape[1]
    height, width = down_master.shape
    tokens = tokens_in.shape[0]
    up_cuts = pieces_of(cols, UNIT, UP_CUTS)
    down_cuts = pieces_of(width, 128, DOWN_CUTS)
    slabs = pieces_of(height, LINE, 8)
    dma = pltpu.SemaphoreType.DMA
    lanes, whole, strip = dma((CORES, up_cuts)), dma((fs, up_cuts)), dma((down_cuts,))
    up_sems = [dma] * 6 + [whole, lanes, whole, dma((up_cuts,))]
    down_sems = [dma] * 8 + [strip] * 4
    sum_sems = [dma, dma((2, down_cuts)), dma, strip]
    vmem = pl.BlockSpec(memory_space=pltpu.VMEM)
    hbm = pl.BlockSpec(memory_space=pl.ANY)
    late = width // down_cuts * LATE
    got_up, got_down, out, base, rest, away = pl.pallas_call(
        functools.partial(hand_over, dims, (up_cuts, down_cuts)),
        out_shape=(
            pltpu.VMEM((fs, groups * CORES, rows, cols), jnp.bfloat16),
            pltpu.VMEM((height, tp * width), jnp.bfloat16),
            pltpu.VMEM((tokens, width - late), jnp.bfloat16),
            pltpu.VMEM((tokens, late), jnp.float32),
            pltpu.VMEM((tokens, late), jnp.float32),
            pltpu.VMEM((tokens, late), jnp.bfloat16),
        ),
        in_specs=[hbm, vmem, hbm, hbm],
        out_specs=(vmem,) * 6,
        scratch_shapes=[
            pltpu.VMEM(tokens_in.shape, jnp.bfloat16),
            pltpu.VMEM((up_master.shape[0], 128), jnp.float32),
            pltpu.VMEM((CORES, rows, cols), jnp.float32),
            pltpu.VMEM((CORES, rows, cols), jnp.bfloat16),
            pltpu.VMEM((CORES, rows, cols), jnp.bfloat16),
            pltpu.VMEM((2, height // slabs, width), jnp.float32),
            pltpu.VMEM((tokens, cols), jnp.bfloat16),
            pltpu.VMEM((tokens, width), jnp.float32),
            pltpu.VMEM((2, tokens, width), jnp.float32),
            pltpu.VMEM((2, tokens, width), jnp.bfloat16),
            pltpu.VMEM((2, tokens, width), jnp.bfloat16),
            pltpu.VMEM((tokens, width), jnp.bfloat16),
            pltpu.VMEM((tokens, width), jnp.bfloat16),
            up_sems,
            down_sems,
            sum_sems,
            [dma((up_cuts,)), dma((2,)), dma],
        ],
        compiler_params=pltpu.CompilerParams(collective_id=0, has_side_effects=True, vmem_limit_bytes=LIMIT << 20),
    )(tokens_in, norm_gain, up_master.reshape(groups * CORES, rows, cols), down_master)
    near = lax.ppermute(away, "fs", [(i, i + 1 - 2 * (i % 2)) for i in range(fs)])
    up = put(got_up).reshape(fs * groups * CORES * rows, cols)
    merged = rest + near.astype(jnp.float32)
    far = lax.ppermute(merged.astype(jnp.bfloat16), "fs", [(i, (i + 2) % fs) for i in range(fs)])
    down = put(got_down)
    home = lax.axis_index("tp") // CORES == lax.axis_index("fs") // CORES
    tail = jnp.where(home, base, merged + far.astype(jnp.float32)).astype(jnp.bfloat16)
    return jnp.concatenate([out, tail], axis=1), up, down


def fits(up_shape, down_shape, dims):
    groups, fs, tp = dims
    own = 2 * (up_shape[0] * up_shape[1] * fs + down_shape[0] * down_shape[1] * tp)
    aligned = up_shape[0] % (groups * CORES * LINE) == 0 and up_shape[0] % 128 == 0 and up_shape[1] % UNIT == 0
    square = groups == 2 and tp == CORES * PLANES and fs == tp
    return square and aligned and down_shape[0] % UNIT == 0 and down_shape[1] % 128 == 0 and own <= 40 << 20 and pieces_of(down_shape[1], 128, DOWN_CUTS) == DOWN_CUTS


def by_collectives(normalized, up_cast, down_cast):
    quarter = lax.all_to_all(up_cast, "tp", split_axis=0, concat_axis=1, tiled=True)
    moved = lax.all_to_all(quarter, "fs", split_axis=1, concat_axis=0, tiled=True)
    part_rows = quarter.shape[0]
    stacked = moved.reshape(moved.shape[0] // part_rows, part_rows, moved.shape[1])
    joined = lax.all_gather(stacked, "tp", axis=1, tiled=True)
    sampled_down = lax.all_gather(down_cast, "tp", axis=1, tiled=True)
    sampled_up = joined.reshape(joined.shape[0] * joined.shape[1], joined.shape[2])
    before = jnp.dot(normalized, sampled_up, preferred_element_type=jnp.float32)
    hidden = jnp.square(jax.nn.relu(before)).astype(jnp.bfloat16)
    terms = jnp.dot(hidden, sampled_down, preferred_element_type=jnp.float32)
    summed = lax.psum_scatter(terms, "fs", scatter_dimension=1, tiled=True)
    return summed.astype(jnp.bfloat16), sampled_up, sampled_down


def shards(dims, tokens, up_master, down_master, norm_gain):
    if fits(up_master.shape, down_master.shape, dims):
        return fused(tokens, up_master, down_master, norm_gain, dims)
    up_cast = (norm_gain[:, None] * up_master).astype(jnp.bfloat16)
    return by_collectives(normalize(tokens), up_cast, down_master.astype(jnp.bfloat16))


def solution(mesh):
    dims = tuple(mesh.shape[name] for name in ("grp", "fs", "tp"))
    return jax.shard_map(
        functools.partial(shards, dims),
        mesh=mesh,
        in_specs=(P(("grp", "tp"), None), P("fs", "tp"), P("fs", "tp"), P("fs")),
        out_specs=(P(("grp", "tp"), "fs"), P("grp", "fs"), P(("grp", "fs"), None)),
        check_vma=False,
    )
```

```python
import functools

import jax
import jax.numpy as jnp
from jax import lax
from jax.experimental import pallas as pl
from jax.experimental.pallas import tpu as pltpu
from jax.sharding import PartitionSpec as P

MESH = pl.DeviceIdType.MESH
CORES = 2
PLANES = 2
LAG = 3
UNIT = 256
LINE = 16
LIMIT = 24
STAGES = 4
DELAY = 3
AHEAD = 2
LATE = 2
EAGER = 2
FLOPS = 10_000_000_000
NORMS = 4
START = 0.12
UP_CUTS = 12
DOWN_CUTS = 6
SHARED = 19
SHARES = 32


def normalize(tokens):
    values = tokens.astype(jnp.float32)
    center = jnp.mean(values, axis=-1, keepdims=True)
    spread = jnp.mean(jnp.square(values - center), axis=-1, keepdims=True)
    return ((values - center) * lax.rsqrt(spread + 1e-05)).astype(jnp.bfloat16)


def pieces_of(size, unit, most):
    for count in range(most, 1, -1):
        if size % (count * unit) == 0:
            return count
    return 1


def shared_rows(height):
    return height * SHARED // SHARES // (2 * LINE) * (2 * LINE)


def order_of(fs, up_cuts, down_cuts, share):
    ready = []
    for cut in range(up_cuts):
        at = (cut + 1) / up_cuts
        ready.append((START + at, 0, "relay", 0, cut))
        for j, came in enumerate((START + at, START + 0.1 + 1.5 * at, START + 0.2 + 1.5 * at, START + 1.15 + at)):
            ready.append((came, 1, "arrive", j, cut))
    for cut in range(down_cuts):
        at = (cut + 1) / down_cuts
        ready.append((START + 1.05 + (1 - share) * at, 2, "split", 0, cut))
        ready.append((START + 1.05 + 1 - share + 2 * share * at, 4, "shared", 0, cut))
    ready.append((START + 0.3, 0, "send", 0, 0))
    ready.append((START + 0.6, 0, "send", 1, 0))
    ready.sort()
    order, spare, now = [], [], START
    for came, _, kind, j, cut in ready:
        while spare and kind == "arrive" and now + (1 - share) / down_cuts <= came:
            order.append(("cross", 0, spare.pop(0)))
            now += (1 - share) / down_cuts
        order.append((kind, j, cut))
        if kind == "arrive":
            now = max(now, came) + 2 / (fs * up_cuts)
        if kind == "split":
            spare.append(cut)
    last = max(i for i, entry in enumerate(order) if entry[0] == "arrive") + 1
    return order[:last], spare


def hand_over(dims, cuts, tokens_ref, gain_ref, up_ref, master_ref, got_up, got_down, out_ref, base_ref, late_ref, away_ref, rows_ref, gains, up_stage, up_src, relayed, stage, hidden, hold, keep, send1, recv1, send2, recv2, up_sems, down_sems, sum_sems, load_sems):
    groups, fs, tp = dims
    up_cuts, down_cuts = cuts
    y, f, t = lax.axis_index("grp"), lax.axis_index("fs"), lax.axis_index("tp")
    x, k = t // CORES, t % CORES
    home_send, cross_send, relay_send, y_send, a_send, b_send, first_recv, relay_recv, y_recv, pair_recv = up_sems
    own_send, own_recv, split_send, shared_send, dy_send, da_send, ds_send, db_send, split_recv, shared_recv, dy_recv, twin_recv = down_sems
    send1_send, send1_recv, send2_send, send2_recv = sum_sems
    load_up, load_down, load_tokens = load_sems
    rows, cols = up_src.shape[1], up_src.shape[2] // up_cuts
    depth = got_up.shape[0] * got_up.shape[1] * got_up.shape[2]
    height, width = master_ref.shape
    tile = width // down_cuts
    both = shared_rows(height)
    part = (height - both) // groups
    near = f + 1 - 2 * (f % 2)
    rows_from = (f, near, (fs - 1) * (1 - f // 2), 2 - f // 2)
    facing = (f + 2) % fs
    sibling = (y, f, x * CORES + (1 - k))
    across_y = (1 - y, f, t)
    other = (1 - x) * CORES
    across_x = (y, f, other + k)

    def remote(src, dst, send, recv, where):
        return pltpu.make_async_remote_copy(src_ref=src, dst_ref=dst, send_sem=send, recv_sem=recv, device_id=where, device_id_type=MESH)

    def up_at(ref, group, lane, cut):
        return ref.at[group * CORES + lane, :, pl.ds(cut * cols, cols)]

    def src_at(lane, cut):
        return up_src.at[lane, :, pl.ds(cut * cols, cols)]

    def up_load(lane, cut):
        at = pl.ds(cut * cols, cols)
        return pltpu.make_async_copy(up_ref.at[y * CORES + lane, :, at], up_stage.at[lane, :, at], load_up.at[cut])

    def up_local(cut):
        return pltpu.make_async_copy(src_at(k, cut), up_at(got_up.at[f], y, k, cut), first_recv.at[f, cut])

    def up_home(lane, cut):
        return remote(src_at(lane, cut), up_at(got_up.at[f], y, lane, cut), home_send, first_recv.at[f, cut], (y, t, x * CORES + lane))

    def up_cross_own(lane, cut):
        return remote(src_at(lane, cut), up_at(got_up.at[f], y, lane, cut), cross_send, first_recv.at[f, cut], (y, f, other + lane))

    def up_cross(lane, cut):
        return remote(src_at(lane, cut), relayed.at[k, :, pl.ds(cut * cols, cols)], cross_send, relay_recv.at[k, cut], (y, f, other + lane))

    def up_relay(slot, cut):
        return remote(relayed.at[slot, :, pl.ds(cut * cols, cols)], up_at(got_up.at[f], y, k, cut), relay_send, first_recv.at[f, cut], (y, other + slot, t))

    def up_here(r, cut):
        return pltpu.make_async_copy(src_at(0, cut), up_at(got_up.at[r], y, k, cut), first_recv.at[r, cut])

    def relay_here(slot, cut):
        return pltpu.make_async_copy(src_at(0, cut), relayed.at[slot, :, pl.ds(cut * cols, cols)], relay_recv.at[slot, cut])

    def up_y(r, cut):
        here = up_at(got_up.at[r], y, k, cut)
        return remote(here, here, y_send, y_recv.at[r, cut], across_y)

    def up_a(r, cut):
        here = up_at(got_up.at[r], y, k, cut)
        return remote(here, here, a_send, pair_recv.at[cut], sibling)

    def up_b(r, cut):
        here = up_at(got_up.at[r], 1 - y, k, cut)
        return remote(here, here, b_send, pair_recv.at[cut], sibling)

    def tile_at(first, size, column, cut):
        return got_down.at[pl.ds(pl.multiple_of(first, LINE), size), pl.ds(pl.multiple_of(column * width + cut * tile, tile), tile)]

    def split_at(group, column, cut):
        return tile_at(group * part, part, column, cut)

    def shared_at(column, cut):
        return tile_at(groups * part, both, column, cut)

    def down_split(cut):
        here = split_at(y, t, cut)
        return remote(here, here, split_send, split_recv.at[cut], across_x)

    def down_shared(cut):
        here = shared_at(t, cut)
        return remote(here, here, shared_send, shared_recv.at[cut], across_x)

    def down_y(cut):
        here = split_at(y, other + k, cut)
        return remote(here, here, dy_send, dy_recv.at[cut], across_y)

    def down_a(cut):
        here = split_at(y, other + k, cut)
        return remote(here, here, da_send, twin_recv.at[cut], sibling)

    def down_s(cut):
        here = shared_at(other + k, cut)
        return remote(here, here, ds_send, twin_recv.at[cut], sibling)

    def down_b(cut):
        here = split_at(1 - y, other + k, cut)
        return remote(here, here, db_send, twin_recv.at[cut], sibling)

    own_columns = got_down.at[:, pl.ds(pl.multiple_of(t * width, width), width)]
    down_own = remote(own_columns, own_columns, own_send, own_recv, sibling)

    slab = stage.shape[1]
    slots = stage.shape[0]
    slabs = height // slab

    def take(step):
        return pltpu.make_async_copy(master_ref.at[pl.ds(step * slab, slab), :], stage.at[step % slots], load_down.at[step % slots])

    take_tokens = pltpu.make_async_copy(tokens_ref, rows_ref, load_tokens)

    for cut in range(up_cuts):
        for lane in range(CORES):
            up_load(lane, cut).start()
    for step in range(slots):
        take(step).start()
    take_tokens.start()

    barrier = pltpu.get_barrier_semaphore()
    partners = [sibling, across_y] + [(y, f, other + lane) for lane in range(CORES)]
    partners += [(y, rows_from[j], x * CORES + lane) for j in range(1, fs) for lane in range(CORES)]
    for partner in partners:
        pl.semaphore_signal(barrier, inc=1, device_id=partner, device_id_type=MESH)

    gains[...] = jnp.transpose(jnp.broadcast_to(gain_ref[...][None, :], (128, gain_ref.shape[0])))

    def up_cast(cut):
        whole = up_stage.at[:, :, pl.ds(cut * cols, cols)]
        pltpu.make_async_copy(whole, whole, load_up.at[cut]).wait()
        for lane in range(CORES):
            @pl.loop(0, rows // LINE)
            def _(line):
                at = pl.ds(pl.multiple_of(line * LINE, LINE), LINE)
                scale = gains[pl.ds(pl.multiple_of((y * CORES + lane) * rows + line * LINE, LINE), LINE), :]
                block = up_stage[lane, at, pl.ds(cut * cols, cols)]
                up_src[lane, at, pl.ds(cut * cols, cols)] = (jnp.concatenate([scale] * (cols // 128), axis=1) * block).astype(jnp.bfloat16)

    def up_start(cut):
        for lane in range(CORES):
            @pl.when(t == f)
            def _():
                up_cross_own(lane, cut).start()

            @pl.when(t != f)
            def _():
                up_cross(lane, cut).start()

    def up_direct(cut):
        for lane in range(CORES):
            @pl.when(jnp.logical_or(t != f, lane != k))
            def _():
                up_home(lane, cut).start()

        @pl.when(t == f)
        def _():
            up_local(cut).start()

    for cut in range(min(EAGER, up_cuts)):
        up_cast(cut)
    pl.semaphore_wait(barrier, len(partners))
    for cut in range(up_cuts):
        if cut >= EAGER:
            up_cast(cut)
        up_start(cut)
        if cut == 0:
            up_direct(cut)

    def down_cast(step):
        take(step).wait()

        @pl.loop(0, slab // LINE)
        def _(line):
            start = pl.multiple_of(line * LINE, LINE)
            to = pl.ds(pl.multiple_of(step * slab + start, LINE), LINE)
            got_down[to, pl.ds(pl.multiple_of(t * width, width), width)] = stage[step % slots, pl.ds(start, LINE), :].astype(jnp.bfloat16)

        if step + slots < slabs:
            take(step + slots).start()
        if step == slabs - 1:
            down_own.start()

    def normalize_rows(step):
        if step == 0:
            take_tokens.wait()
        span = tokens_ref.shape[0] // NORMS

        @pl.loop(0, span // LINE)
        def _(line):
            at = pl.ds(pl.multiple_of(step * span + line * LINE, LINE), LINE)
            rows_ref[at, :] = normalize(rows_ref[at, :])

    def hidden_units(cut):
        @pl.loop(0, cols // UNIT)
        def _(step):
            at = pl.ds(pl.multiple_of(cut * cols + step * UNIT, UNIT), UNIT)
            block = got_up[:, :, :, at].reshape(depth, UNIT)
            before = jnp.dot(rows_ref[...], block, preferred_element_type=jnp.float32)
            hidden[:, at] = jnp.square(jnp.maximum(before, 0.0)).astype(jnp.bfloat16)

    def up_arrive(j, cut):
        r = rows_from[j]
        up_here(r, cut).wait()
        up_y(r, cut).start()
        up_a(r, cut).start()

    def up_second(j, cut):
        r = rows_from[j]
        up_y(r, cut).wait_recv()
        up_b(r, cut).start()

    def up_done(cut):
        landed = got_up.at[:, pl.ds(0, groups), :, pl.ds(cut * cols, cols)]
        pltpu.make_async_copy(landed, landed, pair_recv.at[cut]).wait()
        hidden_units(cut)

    def sum_near(g, cut):
        at = pl.ds(cut * tile, tile)
        return remote(send1.at[g, :, at], recv1.at[g, :, at], send1_send, send1_recv.at[g, cut], (y, near, t))

    def sum_far(cut):
        at = pl.ds(cut * tile, tile)
        return remote(send2.at[:, at], recv2.at[:, at], send2_send, send2_recv.at[cut], (y, facing, t))

    bases = (x * CORES, other)
    soon = down_cuts - LATE
    close = x == f // CORES
    kept = (x + f // CORES) % PLANES

    def terms(g, cut, first, last):
        away, here = (pl.ds(pl.multiple_of(column * width + cut * tile, tile), tile) for column in (bases[g] + 1 - f % 2, bases[g] + f % 2))
        total = jnp.zeros((hidden.shape[0], 2 * tile), jnp.float32)
        for unit in range(first, last, UNIT):
            at = pl.ds(unit, UNIT)
            block = jnp.concatenate([got_down[at, away], got_down[at, here]], axis=1)
            total += jnp.dot(hidden[:, at], block, preferred_element_type=jnp.float32)
        return total[:, :tile], total[:, tile:]

    def features(g, cut, first, last):
        at = pl.ds(cut * tile, tile)
        away, here = terms(g, cut, first, last)
        if g == 1 and cut >= soon:
            place = pl.ds((cut - soon) * tile, tile)
            late_ref[:, place] = here
            away_ref[:, place] = away.astype(jnp.bfloat16)
            return
        if first > 0:
            away, here = hold[:, at] + away, keep[g, :, at] + here
        keep[g, :, at] = here
        if last == height:
            send1[g, :, at] = away.astype(jnp.bfloat16)
            if g == 1 or cut < AHEAD:
                sum_near(g, cut).start()
            else:
                @pl.when(jnp.logical_not(close))
                def _():
                    sum_near(g, cut).start()
        else:
            hold[:, at] = away

    def pass_on(g, cut):
        at = pl.ds(cut * tile, tile)
        sum_near(g, cut).wait_recv()
        send2[:, at] = (keep[g, :, at] + recv1[g, :, at].astype(jnp.float32)).astype(jnp.bfloat16)
        sum_far(cut).start()

    def finish(cut):
        at = pl.ds(cut * tile, tile)
        sum_near(kept, cut).wait_recv()
        sum_far(cut).wait_recv()
        total = keep[kept, :, at] + recv1[kept, :, at].astype(jnp.float32) + recv2[:, at].astype(jnp.float32)
        if cut < soon:
            out_ref[:, at] = total.astype(jnp.bfloat16)
        else:
            base_ref[:, pl.ds((cut - soon) * tile, tile)] = total

    def twin_in(cut):
        landed = tile_at(0, height, other + (1 - k), cut)
        pltpu.make_async_copy(landed, landed, twin_recv.at[cut]).wait()

    def sent(ref, sem):
        pltpu.make_async_copy(ref, ref, sem).wait()

    def drain():
        sent(up_src, cross_send)

        @pl.when(t == f)
        def _():
            sent(up_src.at[0], home_send)

        @pl.when(t != f)
        def _():
            sent(up_src, home_send)

        @pl.when(jnp.logical_or(other == f, other + 1 == f))
        def _():
            sent(relayed.at[0], relay_send)

        @pl.when(jnp.logical_and(other != f, other + 1 != f))
        def _():
            sent(relayed, relay_send)

        for sem in (y_send, a_send, b_send):
            sent(got_up.at[:, 0], sem)
        sent(own_columns, own_send)
        for sem in (split_send, dy_send, da_send, db_send):
            sent(got_down.at[pl.ds(0, part), pl.ds(0, width)], sem)
        for sem in (shared_send, ds_send):
            sent(got_down.at[pl.ds(0, both), pl.ds(0, width)], sem)

    waiting, seen, ready, crossed, shared = [], [0] * up_cuts, [], [], []
    tasks = [functools.partial(down_cast, step) for step in range(slabs)] + [functools.partial(normalize_rows, step) for step in range(NORMS)]
    stages = STAGES if up_cuts % STAGES == 0 and height == up_cuts * cols else 1
    span = up_cuts // stages

    def finished(cut):
        up_done(cut)
        if (cut + 1) % span == 0 and cut + 1 < up_cuts:
            if cut + 1 == span:
                tasks.append(down_own.wait_recv)
            for piece in range(down_cuts):
                tasks.append(functools.partial(features, 0, piece, (cut + 1 - span) * cols, (cut + 1) * cols))

    def spend(count):
        for _ in range(min(count, len(tasks))):
            tasks.pop(0)()

    def follow():
        kind, j, cut = waiting.pop(0)
        if kind == "cross":
            down_y(cut).wait_recv()
            down_b(cut).start()
            crossed.append(cut)
        else:
            up_second(j, cut)
            seen[cut] += 1
            if seen[cut] == fs:
                ready.append(cut)

    def shared_in(cut):
        down_shared(cut).wait_recv()
        down_s(cut).start()
        shared.append(cut)

    order, late = order_of(fs, up_cuts, down_cuts, both / height)
    for kind, j, cut in order:
        if kind == "relay":
            for slot in range(CORES):
                @pl.when(other + slot != f)
                def _():
                    relay_here(slot, cut).wait()
                    up_relay(slot, cut).start()

            if cut + 1 < up_cuts:
                up_direct(cut + 1)
            spend(1)
        elif kind == "send":
            if j == 0:
                spend(len(tasks))
            for piece in range(down_cuts):
                (down_split, down_shared)[j](piece).start()
        elif kind == "split":
            down_split(cut).wait_recv()
            down_a(cut).start()
        elif kind == "shared":
            shared_in(cut)
        else:
            if kind == "cross":
                down_y(cut).start()
            else:
                up_arrive(j, cut)
            waiting.append((kind, j, cut))
            if len(waiting) > LAG:
                follow()
            if len(ready) > 1:
                finished(ready.pop(0))
            else:
                spend(1)

    for cut in late:
        down_y(cut).start()
        waiting.append(("cross", 0, cut))
    while sum(seen) < fs * up_cuts:
        follow()
        spend(2)
        while ready:
            finished(ready.pop(0))
    spend(len(tasks))
    if stages == 1:
        down_own.wait_recv()
    for cut in range(down_cuts):
        features(0, cut, height - height // stages, height)

    def cross_in(step):
        while step not in crossed:
            follow()

    for step in range(down_cuts):
        if step not in shared:
            shared_in(step)
        cross_in(step)
        @pl.when(jnp.logical_not(close))
        def _():
            pass_on(0, step)

        if DELAY <= step < DELAY + soon:
            @pl.when(close)
            def _():
                pass_on(1, step - DELAY)

        twin_in(step)
        features(1, step, 0, height)
        if step + AHEAD < down_cuts:
            @pl.when(close)
            def _():
                sum_near(0, step + AHEAD).start()

    @pl.when(close)
    def _():
        for step in range(max(down_cuts - DELAY, 0), soon):
            pass_on(1, step)

    drain()
    for step in range(soon):
        finish(step)

    sent(rows_ref.at[:, pl.ds(0, (down_cuts + soon) * tile)], send1_send)

    @pl.when(close)
    def _():
        for step in range(soon, down_cuts):
            finish(step)
        if soon:
            sent(send2.at[:, pl.ds(0, soon * tile)], send2_send)

    @pl.when(jnp.logical_not(close))
    def _():
        base_ref[...] = jnp.zeros_like(base_ref)
        sent(send2, send2_send)


def put_out(src_ref, out_ref, sems):
    chunks = sems.shape[0]
    step = src_ref.shape[0] // chunks
    for chunk in range(chunks):
        at = pl.ds(chunk * step, step)
        pltpu.make_async_copy(src_ref.at[at], out_ref.at[at], sems.at[chunk]).start()
    for chunk in range(chunks):
        at = pl.ds(chunk * step, step)
        pltpu.make_async_copy(src_ref.at[at], out_ref.at[at], sems.at[chunk]).wait()


def put(array):
    return pl.pallas_call(
        put_out,
        out_shape=jax.ShapeDtypeStruct(array.shape, array.dtype),
        in_specs=[pl.BlockSpec(memory_space=pltpu.VMEM)],
        out_specs=pl.BlockSpec(memory_space=pltpu.HBM),
        scratch_shapes=[pltpu.SemaphoreType.DMA((4,))],
        compiler_params=pltpu.CompilerParams(vmem_limit_bytes=1 << 20),
        cost_estimate=pl.CostEstimate(flops=FLOPS, bytes_accessed=2 * array.size, transcendentals=0),
    )(array)


def fused(tokens_in, up_master, down_master, norm_gain, dims):
    groups, fs, tp = dims
    rows, cols = up_master.shape[0] // (groups * CORES), up_master.shape[1]
    height, width = down_master.shape
    tokens = tokens_in.shape[0]
    up_cuts = pieces_of(cols, UNIT, UP_CUTS)
    down_cuts = pieces_of(width, 128, DOWN_CUTS)
    slabs = pieces_of(height, LINE, 8)
    dma = pltpu.SemaphoreType.DMA
    lanes, whole, strip = dma((CORES, up_cuts)), dma((fs, up_cuts)), dma((down_cuts,))
    up_sems = [dma] * 6 + [whole, lanes, whole, dma((up_cuts,))]
    down_sems = [dma] * 8 + [strip] * 4
    sum_sems = [dma, dma((2, down_cuts)), dma, strip]
    vmem = pl.BlockSpec(memory_space=pltpu.VMEM)
    hbm = pl.BlockSpec(memory_space=pl.ANY)
    late = width // down_cuts * LATE
    got_up, got_down, out, base, rest, away = pl.pallas_call(
        functools.partial(hand_over, dims, (up_cuts, down_cuts)),
        out_shape=(
            pltpu.VMEM((fs, groups * CORES, rows, cols), jnp.bfloat16),
            pltpu.VMEM((height, tp * width), jnp.bfloat16),
            pltpu.VMEM((tokens, width - late), jnp.bfloat16),
            pltpu.VMEM((tokens, late), jnp.float32),
            pltpu.VMEM((tokens, late), jnp.float32),
            pltpu.VMEM((tokens, late), jnp.bfloat16),
        ),
        in_specs=[hbm, vmem, hbm, hbm],
        out_specs=(vmem,) * 6,
        scratch_shapes=[
            pltpu.VMEM(tokens_in.shape, jnp.bfloat16),
            pltpu.VMEM((up_master.shape[0], 128), jnp.float32),
            pltpu.VMEM((CORES, rows, cols), jnp.float32),
            pltpu.VMEM((CORES, rows, cols), jnp.bfloat16),
            pltpu.VMEM((CORES, rows, cols), jnp.bfloat16),
            pltpu.VMEM((2, height // slabs, width), jnp.float32),
            pltpu.VMEM((tokens, cols), jnp.bfloat16),
            pltpu.VMEM((tokens, width), jnp.float32),
            pltpu.VMEM((2, tokens, width), jnp.float32),
            pltpu.VMEM((2, tokens, width), jnp.bfloat16),
            pltpu.VMEM((2, tokens, width), jnp.bfloat16),
            pltpu.VMEM((tokens, width), jnp.bfloat16),
            pltpu.VMEM((tokens, width), jnp.bfloat16),
            up_sems,
            down_sems,
            sum_sems,
            [dma((up_cuts,)), dma((2,)), dma],
        ],
        compiler_params=pltpu.CompilerParams(collective_id=0, has_side_effects=True, vmem_limit_bytes=LIMIT << 20),
    )(tokens_in, norm_gain, up_master.reshape(groups * CORES, rows, cols), down_master)
    near = lax.ppermute(away, "fs", [(i, i + 1 - 2 * (i % 2)) for i in range(fs)])
    up = put(got_up).reshape(fs * groups * CORES * rows, cols)
    merged = rest + near.astype(jnp.float32)
    far = lax.ppermute(merged.astype(jnp.bfloat16), "fs", [(i, (i + 2) % fs) for i in range(fs)])
    down = put(got_down)
    home = lax.axis_index("tp") // CORES == lax.axis_index("fs") // CORES
    tail = jnp.where(home, base, merged + far.astype(jnp.float32)).astype(jnp.bfloat16)
    return jnp.concatenate([out, tail], axis=1), up, down


def fits(up_shape, down_shape, dims):
    groups, fs, tp = dims
    own = 2 * (up_shape[0] * up_shape[1] * fs + down_shape[0] * down_shape[1] * tp)
    aligned = up_shape[0] % (groups * CORES * LINE) == 0 and up_shape[0] % 128 == 0 and up_shape[1] % UNIT == 0
    square = groups == 2 and tp == CORES * PLANES and fs == tp
    return square and aligned and down_shape[0] % UNIT == 0 and down_shape[1] % 128 == 0 and own <= 40 << 20 and pieces_of(down_shape[1], 128, DOWN_CUTS) == DOWN_CUTS


def by_collectives(normalized, up_cast, down_cast):
    quarter = lax.all_to_all(up_cast, "tp", split_axis=0, concat_axis=1, tiled=True)
    moved = lax.all_to_all(quarter, "fs", split_axis=1, concat_axis=0, tiled=True)
    part_rows = quarter.shape[0]
    stacked = moved.reshape(moved.shape[0] // part_rows, part_rows, moved.shape[1])
    joined = lax.all_gather(stacked, "tp", axis=1, tiled=True)
    sampled_down = lax.all_gather(down_cast, "tp", axis=1, tiled=True)
    sampled_up = joined.reshape(joined.shape[0] * joined.shape[1], joined.shape[2])
    before = jnp.dot(normalized, sampled_up, preferred_element_type=jnp.float32)
    hidden = jnp.square(jax.nn.relu(before)).astype(jnp.bfloat16)
    terms = jnp.dot(hidden, sampled_down, preferred_element_type=jnp.float32)
    summed = lax.psum_scatter(terms, "fs", scatter_dimension=1, tiled=True)
    return summed.astype(jnp.bfloat16), sampled_up, sampled_down


def shards(dims, tokens, up_master, down_master, norm_gain):
    if fits(up_master.shape, down_master.shape, dims):
        return fused(tokens, up_master, down_master, norm_gain, dims)
    up_cast = (norm_gain[:, None] * up_master).astype(jnp.bfloat16)
    return by_collectives(normalize(tokens), up_cast, down_master.astype(jnp.bfloat16))


def solution(mesh):
    dims = tuple(mesh.shape[name] for name in ("grp", "fs", "tp"))
    return jax.shard_map(
        functools.partial(shards, dims),
        mesh=mesh,
        in_specs=(P(("grp", "tp"), None), P("fs", "tp"), P("fs", "tp"), P("fs")),
        out_specs=(P(("grp", "tp"), "fs"), P("grp", "fs"), P(("grp", "fs"), None)),
        check_vma=False,
    )
```
